256 devices in a mesh: sp: 32 (over z, x), tp: 8 (over y, core).
Axes of the slice: x: 4, y: 4, z: 8, core: 2. Of those that a mesh axis runs over, the one named last changes fastest.
Arguments:
- tokens: bfloat16 [32768, 2048], P('sp'), may hold values from -6 to 6
- pre_gain: float32 [2048], replicated, may hold values from 0.1 to 1.9
- w_query: bfloat16 [2048, 2048], P(None, 'tp'), may hold values from -0.125 to 0.125
- w_key: bfloat16 [2048, 2048], P(None, 'tp'), may hold values from -0.125 to 0.125
- w_value: bfloat16 [2048, 2048], P(None, 'tp'), may hold values from -0.125 to 0.125
- memory_output_gate_weight: bfloat16 [2048, 2048], P(None, 'tp'), may hold values from -0.125 to 0.125
- w_input_gate: bfloat16 [2048, 8], replicated, may hold values from -0.125 to 0.125
- w_forget_gate: bfloat16 [2048, 8], replicated, may hold values from -0.125 to 0.125
- input_bias: float32 [8], replicated, may hold values from -3 to 220
- forget_bias: float32 [8], replicated, may hold values from 3.9 to 12.4
- forget_extra: float32 [32768, 8], P('sp', 'tp'), may hold values from -1.5 to 0
- initial_memory: float32 [8, 256, 256], P('tp', 'sp'), may hold values from -4096 to 4096
- initial_normal: float32 [8, 256], P('tp', 'sp'), may hold values from -4096 to 4096
- memory_gain: float32 [2048], replicated, may hold values from 0.1 to 1.9
- w_pool_input: bfloat16 [2048, 1024], P(None, 'tp'), may hold values from -0.125 to 0.125
- w_pool_gate: bfloat16 [2048, 1024], P(None, 'tp'), may hold values from -0.125 to 0.125
- pool_mix: bfloat16 [8, 128, 128], replicated, may hold values from -0.5 to 0.5
- pool_gain: float32 [1024], replicated, may hold values from 0.1 to 1.9
- w_out_memory: bfloat16 [2048, 2048], P('tp'), may hold values from -0.109375 to 0.109375
- w_out_pool: bfloat16 [1024, 2048], P('tp'), may hold values from -0.109375 to 0.109375
- post_gain: float32 [2048], replicated, may hold values from 0.1 to 1.9
Outputs:
- layer_out: bfloat16 [32768, 2048], P(('sp', 'tp'))
The draws below stay inside these ranges and needn't reach their ends.
All inputs are finite; a program needn't handle non-finite values.
Results may differ from the reference program's by a relative error of at most 0.018.
The reference program's roundings to bfloat16 on the way count: a program that leaves them out, or rounds other values in their place, can miss the bound.
Values may be sent and summed in bfloat16 or wider, within the bound.
A program may use at most 128 MiB of HBM per device.

```python
import jax
import jax.numpy as jnp
from jax import lax

D = 2048
HEADS = 8
HEAD_DIM = 256
MEM_WIDTH = 2048
POOL_GROUPS = 8
GROUP_DIM = 128
POOL_WIDTH = 1024
TOKENS_PER_SHARD = 1024
BLOCK = 512
TOKENS = 32768
N_TP = 8


def draw_input_bias(key, part):
    result = jnp.clip(jax.random.normal(jax.random.fold_in(key, 13), (HEADS,), jnp.float32), -3.0, 3.0)
    return result


def draw_forget_bias(key, part):
    order = jax.random.permutation(jax.random.fold_in(key, 21), HEADS)
    fast_count = HEADS // 2
    slow_value = jnp.log(jnp.float32(TOKENS)) + 1.5 + jax.random.uniform(jax.random.fold_in(key, 22), (HEADS,), jnp.float32, -0.5, 0.5)
    slow_value = jnp.minimum(slow_value, 12.4)
    fast_value = jax.random.uniform(jax.random.fold_in(key, 23), (HEADS,), jnp.float32, 3.9, 4.6)
    return jnp.where(order < fast_count, fast_value, slow_value)


def draw_forget_extra(key, part):
    block_total = TOKENS // TOKENS_PER_SHARD
    rates = jnp.exp(jax.random.uniform(jax.random.fold_in(key, 31), (block_total, HEADS), jnp.float32, jnp.log(0.3), jnp.log(1.2)))
    rough = jax.random.uniform(jax.random.fold_in(key, 32), (TOKENS, HEADS), jnp.float32, 0.5, 1.5)
    baseline = -(jnp.repeat(rates, TOKENS_PER_SHARD, axis=0) * rough) / TOKENS
    spots = jax.random.randint(jax.random.fold_in(key, 33), (2,), 0, TOKENS)
    losses = jax.random.uniform(jax.random.fold_in(key, 34), (2, HEADS), jnp.float32, 0.22, 0.69)
    struck = (jnp.arange(TOKENS)[:, None] == spots[None, :]).astype(jnp.float32)
    return baseline - jnp.dot(struck, losses)


def block_scale(key, shape, pieces, least, top_value):
    def one(dim, parts):
        heights = jax.random.uniform(jax.random.fold_in(jax.random.fold_in(key, 6), dim), (parts,), jnp.float32, least / len(pieces), top_value / len(pieces))
        return jnp.repeat(jnp.exp(heights), shape[dim] // parts).reshape((-1,) + (1,) * (len(shape) - dim - 1))

    factor_of = one(*pieces[0])
    for cut in pieces[1:]:
        factor_of = factor_of * one(*cut)
    return factor_of


def scatter_about(own_key, shape, deviation, limit, shards=(), dtype=jnp.bfloat16):
    values = deviation * jax.random.normal(own_key, shape, jnp.float32)
    if shards:
        values = values * block_scale(own_key, shape, shards, -0.22, 0.18)
    return jnp.clip(values, -limit, limit).astype(dtype)


def setup_inputs(seed: int = 0) -> dict:
    streams_of = jax.random.split(jax.random.key(seed), 22)
    tokens = scatter_about(streams_of[0], (TOKENS, D), 1.0, 6.0, ((0, 32),))
    pre_gain = jnp.clip(1.0 + 0.18 * jax.random.normal(streams_of[1], (D,), jnp.float32), 0.1, 1.9)
    w_query = scatter_about(streams_of[2], (D, MEM_WIDTH), D ** -0.5, 0.125, ((1, 8),))
    w_key = scatter_about(streams_of[3], (D, MEM_WIDTH), D ** -0.5, 0.125, ((1, 8),))
    w_value = scatter_about(streams_of[4], (D, MEM_WIDTH), D ** -0.5, 0.125, ((1, 8),))
    memory_output_gate_weight = scatter_about(streams_of[5], (D, MEM_WIDTH), D ** -0.5, 0.125, ((1, 8),))
    w_input_gate = scatter_about(streams_of[6], (D, HEADS), D ** -0.5, 0.125)
    w_forget_gate = scatter_about(streams_of[7], (D, HEADS), D ** -0.5, 0.125)
    input_bias = draw_input_bias(jax.random.fold_in(streams_of[21], 71), 0)
    forget_bias = draw_forget_bias(jax.random.fold_in(streams_of[21], 71), 0)
    forget_extra = draw_forget_extra(jax.random.fold_in(streams_of[21], 71), 0)
    initial_memory = scatter_about(streams_of[11], (HEADS, HEAD_DIM, HEAD_DIM), (4 * TOKENS ** 0.5), 4096.0, ((0, 8), (1, 32)), jnp.float32)
    initial_normal = scatter_about(streams_of[12], (HEADS, HEAD_DIM), (4 * TOKENS ** 0.5), 4096.0, ((0, 8), (1, 32)), jnp.float32)
    memory_gain = jnp.clip(1.0 + 0.18 * jax.random.normal(streams_of[13], (MEM_WIDTH,), jnp.float32), 0.1, 1.9)
    w_pool_input = scatter_about(streams_of[14], (D, POOL_WIDTH), D ** -0.5, 0.125, ((1, 8),))
    w_pool_gate = scatter_about(streams_of[15], (D, POOL_WIDTH), D ** -0.5, 0.125, ((1, 8),))
    pool_mix = scatter_about(streams_of[16], (POOL_GROUPS, GROUP_DIM, GROUP_DIM), GROUP_DIM ** -0.5, 0.5)
    pool_gain = jnp.clip(1.0 + 0.18 * jax.random.normal(streams_of[17], (POOL_WIDTH,), jnp.float32), 0.1, 1.9)
    w_out_memory = scatter_about(streams_of[18], (MEM_WIDTH, D), (MEM_WIDTH + POOL_WIDTH) ** -0.5, 0.109375, ((0, 8),))
    w_out_pool = scatter_about(streams_of[19], (POOL_WIDTH, D), (MEM_WIDTH + POOL_WIDTH) ** -0.5, 0.109375, ((0, 8),))
    post_gain = jnp.clip(1.0 + 0.18 * jax.random.normal(streams_of[20], (D,), jnp.float32), 0.1, 1.9)
    return dict(tokens=tokens, pre_gain=pre_gain, w_query=w_query, w_key=w_key, w_value=w_value, memory_output_gate_weight=memory_output_gate_weight, w_input_gate=w_input_gate, w_forget_gate=w_forget_gate, input_bias=input_bias, forget_bias=forget_bias, forget_extra=forget_extra, initial_memory=initial_memory, initial_normal=initial_normal, memory_gain=memory_gain, w_pool_input=w_pool_input, w_pool_gate=w_pool_gate, pool_mix=pool_mix, pool_gain=pool_gain, w_out_memory=w_out_memory, w_out_pool=w_out_pool, post_gain=post_gain)


EPS = 1e-06

def normalize(values, gain):
    return values * lax.rsqrt(lax.optimization_barrier(jnp.mean(values * values, axis=-1, keepdims=True)) + EPS) * gain

def block_parts(memory_carry, block_inputs):
    matrix_memory_state, memory_normal, stabilizer = memory_carry
    queries, keys_in, incoming_values, log_input, log_keep = block_inputs
    length = queries.shape[1]
    head_scale = queries.shape[2] ** (-0.5)
    causal = jnp.arange(length)[:, None] >= jnp.arange(length)[None, :]
    running_keep = jnp.cumsum(log_keep, axis=-1)
    decayed = jnp.where(causal[None], running_keep[:, :, None] - running_keep[:, None, :] + log_input[:, None, :], -jnp.inf)
    carried = running_keep + stabilizer[:, None]
    row_max = jnp.maximum(lax.optimization_barrier(jnp.max(decayed, axis=-1)), carried)
    wide_queries = queries.astype(jnp.float32)
    broadcast_values = incoming_values.astype(jnp.float32)
    wide_keys = keys_in.astype(jnp.float32)
    scores = jnp.einsum('hld,hsd->hls', wide_queries, wide_keys)
    weights = jnp.exp(decayed - row_max[:, :, None]) * scores * head_scale
    carry_weight = jnp.exp(carried - row_max) * head_scale
    rounded = lax.optimization_barrier(weights.astype(jnp.bfloat16)).astype(jnp.float32)
    numerator = jnp.einsum('hls,hsd->hld', rounded, broadcast_values)
    numerator = numerator + carry_weight[:, :, None] * jnp.einsum('hld,hde->hle', wide_queries, matrix_memory_state, precision=lax.Precision.HIGHEST)
    denominator = lax.optimization_barrier(jnp.sum(weights, axis=-1)) + carry_weight * jnp.einsum('hld,hd->hl', wide_queries, memory_normal, precision=lax.Precision.HIGHEST)
    block_keep = running_keep[:, -1]
    write_log = block_keep[:, None] - running_keep + log_input
    new_stabilizer = jnp.maximum(block_keep + stabilizer, lax.optimization_barrier(jnp.max(write_log, axis=-1)))
    decay_factor = jnp.exp(block_keep + stabilizer - new_stabilizer)
    write_weight = jnp.exp(write_log - new_stabilizer[:, None])
    key_projected = write_weight[:, :, None] * wide_keys
    key_projected_rounded = lax.optimization_barrier(key_projected.astype(jnp.bfloat16)).astype(jnp.float32)
    matrix_memory_state = decay_factor[:, None, None] * matrix_memory_state + jnp.einsum('gbq,gbd->gqd', key_projected_rounded, broadcast_values)
    memory_normal = decay_factor[:, None] * memory_normal + lax.optimization_barrier(jnp.sum(key_projected, axis=1))
    return ((matrix_memory_state, memory_normal, new_stabilizer), (numerator, denominator, row_max))

def reference(tokens, pre_gain, w_query, w_key, w_value, memory_output_gate_weight, w_input_gate, w_forget_gate, input_bias, forget_bias, forget_extra, initial_memory, initial_normal, memory_gain, w_pool_input, w_pool_gate, pool_mix, pool_gain, w_out_memory, w_out_pool, post_gain):
    normed = normalize(tokens.astype(jnp.float32), pre_gain).astype(jnp.bfloat16)

    def by_heads(weight):
        product = jnp.dot(normed, weight, preferred_element_type=jnp.float32)
        return product.reshape(TOKENS, HEADS, HEAD_DIM).transpose(1, 0, 2)
    queries = by_heads(w_query).astype(jnp.bfloat16)
    keys_all = by_heads(w_key).astype(jnp.bfloat16)
    values_all = by_heads(w_value).astype(jnp.bfloat16)
    memory_gate = by_heads(memory_output_gate_weight)
    log_input = (jnp.dot(normed, w_input_gate, preferred_element_type=jnp.float32) + input_bias).T
    log_keep = (jax.nn.log_sigmoid(jnp.dot(normed, w_forget_gate, preferred_element_type=jnp.float32) + forget_bias) + forget_extra).T
    block_total = TOKENS // BLOCK

    def split(array):
        return jnp.moveaxis(array.reshape((HEADS, block_total, BLOCK) + array.shape[2:]), 1, 0)

    def join(array):
        return jnp.moveaxis(array, 0, 1).reshape((HEADS, TOKENS) + array.shape[3:])
    begin = (initial_memory, initial_normal, jnp.zeros((HEADS,), jnp.float32))
    _, (numerator, denominator, row_max) = lax.scan(block_parts, begin, (split(queries), split(keys_all), split(values_all), split(log_input), split(log_keep)))
    numerator, denominator, row_max = (join(numerator), join(denominator), join(row_max))
    memory_rows = numerator / jnp.maximum(jnp.abs(denominator), jnp.exp(-row_max))[..., None]
    row_scale = lax.rsqrt(lax.optimization_barrier(jnp.mean(memory_rows * memory_rows, axis=(0, 2), keepdims=True)) + EPS)
    memory_out = (memory_rows * row_scale * memory_gain.reshape(HEADS, 1, HEAD_DIM) * jax.nn.silu(memory_gate)).astype(jnp.bfloat16)
    memory_out = memory_out.transpose(1, 0, 2).reshape(TOKENS, MEM_WIDTH)
    pool_input = jnp.dot(normed, w_pool_input, preferred_element_type=jnp.float32).astype(jnp.bfloat16)
    grouped = pool_input.astype(jnp.float32).reshape(TOKENS, POOL_GROUPS, GROUP_DIM)
    running = jnp.concatenate([jnp.zeros((1, POOL_GROUPS, GROUP_DIM), jnp.float32), jnp.cumsum(grouped, axis=0)], axis=0)
    position = (jnp.arange(TOKENS) + 1).astype(jnp.int32)[:, None]
    windows = (2 ** (jnp.arange(POOL_GROUPS) + 1)).astype(jnp.int32)[None, :]
    lowest = jnp.maximum(position - windows, 0).astype(jnp.int32)
    group_ids = jnp.arange(POOL_GROUPS).astype(jnp.int32)[None, :]
    window_sums = running[1:] - running[lowest, group_ids]
    counts = (position - lowest).astype(jnp.float32)
    pooled = (window_sums / counts[..., None] - grouped).astype(jnp.bfloat16)
    mixed = jnp.einsum('tgc,gce->tge', pooled.astype(jnp.float32), pool_mix.astype(jnp.float32))
    pool_gate = jnp.dot(normed, w_pool_gate, preferred_element_type=jnp.float32)
    pool_out = (mixed.reshape(TOKENS, POOL_WIDTH) * pool_gain * jax.nn.silu(pool_gate)).astype(jnp.bfloat16)
    memory_cols = MEM_WIDTH // N_TP
    pool_cols = POOL_WIDTH // N_TP
    summed = jnp.zeros((TOKENS, D), jnp.float32)
    for member in range(N_TP):
        low_mem = member * memory_cols
        low_pool = member * pool_cols
        partial_value = jnp.dot(memory_out[:, low_mem:low_mem + memory_cols], w_out_memory[low_mem:low_mem + memory_cols], preferred_element_type=jnp.float32)
        partial_value = partial_value + jnp.dot(pool_out[:, low_pool:low_pool + pool_cols], w_out_pool[low_pool:low_pool + pool_cols], preferred_element_type=jnp.float32)
        summed = summed + lax.optimization_barrier(partial_value.astype(jnp.bfloat16)).astype(jnp.float32)
    return normalize(summed, post_gain).astype(jnp.bfloat16)
```

```python
import jax
import jax.numpy as jnp
from jax import lax
from jax.experimental import pallas as pl
from jax.experimental.pallas import tpu as pltpu
from jax.sharding import PartitionSpec as P

EPS = 1e-6
NEG = -1e30
F32 = jnp.float32
BF16 = jnp.bfloat16
MESH = pl.DeviceIdType.MESH

T = 1024
D = 2048
H = 256
G = 128
NSP = 32
NZ, NX = 8, 4
NTP = 8
NY = 4
HALO = 256


def nn(a, b):
    return jnp.dot(a, b, preferred_element_type=F32)


def nt(a, b):
    return lax.dot_general(a, b, (((1,), (1,)), ((), ())), preferred_element_type=F32)


def tn(a, b):
    return lax.dot_general(a, b, (((0,), (0,)), ((), ())), preferred_element_type=F32)


def silu(x):
    return x / (1.0 + jnp.exp(-x))


def scan_packed(x, combine, fill):
    lane = lax.broadcasted_iota(jnp.int32, (8, 128), 1)
    sub = lax.broadcasted_iota(jnp.int32, (8, 128), 0)
    for step in (1, 2, 4, 8, 16, 32, 64):
        x = combine(x, jnp.where(lane >= step, pltpu.roll(x, step, 1), fill))
    rows = jnp.broadcast_to(x[:, 127:128], (8, 128))
    before = jnp.where(sub >= 1, pltpu.roll(rows, 1, 0), fill)
    for step in (1, 2, 4):
        before = combine(before, jnp.where(sub >= step, pltpu.roll(before, step, 0), fill))
    return combine(x, before)


def columns_of(packed):
    rows = jnp.concatenate(packed + [jnp.zeros((128 - 8 * len(packed), 128), F32)], axis=0)
    return rows.T


def kernel(
    tokens, pre_gain, w_query, w_key, w_value, w_gate, w_in, w_forget, in_bias, forget_bias, extra, init_memory,
    init_normal, memory_gain, w_pool_in, w_pool_gate, pool_mix, pool_gain, w_out_memory, w_out_pool, post_gain,
    out,
    tok, nrm, wq, wk, wv, wg, wp, gw, pre, bias_i, bias_f, fex, im, inn, mg, pm, pg, wom, wop, post,
    gz, q, k, v, gate, pool_ext, pgate, num, den, cols,
    ustate, usend, urecv, bsend, brecv, ssend, srecv, smat,
    sqs, sqr, zbuf, zsib, part, fwd, r1, r2, r3, r4, r5, r6, obuf,
    lsem, tsem, osem, wsend, wrecv, usem, bsem, hsem, ssem, qsem, zsem, rsend, rrecv,
):
    sp = lax.axis_index("sp")
    tp = lax.axis_index("tp")
    z, x = sp // NX, sp % NX
    y, c = tp // 2, tp % 2
    sib = {"sp": sp, "tp": 2 * y + (1 - c)}
    up = {"sp": sp, "tp": 2 * lax.rem(y + 1, NY) + c}
    down = {"sp": sp, "tp": 2 * lax.rem(y + NY - 1, NY) + c}

    def sp_peer(n):
        kz = n // NX
        dz = lax.rem(4 + (kz + 1) // 2 * (1 - 2 * lax.rem(kz, 2)) + NZ, NZ)
        dx = lax.rem(2 + lax.rem(n, NX), NX)
        dx = jnp.where(lax.rem(n, NX) == 1, 1, jnp.where(lax.rem(n, NX) == 2, 3, jnp.where(lax.rem(n, NX) == 3, 0, 2)))
        return lax.rem(z + dz, NZ) * NX + lax.rem(x + dx, NX)

    barrier = pltpu.get_barrier_semaphore()

    def greet_sp(n, carry):
        pl.semaphore_signal(barrier, inc=1, device_id={"sp": sp_peer(n), "tp": tp}, device_id_type=MESH)
        return carry

    def greet_tp(n, carry):
        pl.semaphore_signal(barrier, inc=1, device_id={"sp": sp, "tp": lax.rem(tp + n, NTP)}, device_id_type=MESH)
        return carry

    lax.fori_loop(0, NSP - 1, greet_sp, 0)
    lax.fori_loop(1, NTP, greet_tp, 0)

    tok_copies = [
        pltpu.make_async_copy(tokens.at[pl.ds(256 * i, 256)], tok.at[pl.ds(256 * i, 256)], tsem.at[i]) for i in range(4)
    ]
    loads = [
        (pre_gain, pre), (w_key, wk), (w_value, wv), (w_in, gw.at[pl.ds(0, 8)]), (w_forget, gw.at[pl.ds(8, 8)]),
        (in_bias, bias_i), (forget_bias, bias_f), (extra, fex), (init_memory, im), (init_normal, inn),
        (w_query, wq), (w_gate, wg), (w_pool_in, wp.at[:, pl.ds(0, G)]), (w_pool_gate, wp.at[:, pl.ds(G, G)]),
        (memory_gain.at[:, pl.ds(pl.multiple_of(tp * H, H), H)], mg), (pool_mix.at[tp], pm),
        (pool_gain.at[:, pl.ds(pl.multiple_of(tp * G, G), G)], pg),
        (w_out_memory, wom.at[pl.ds(0, H)]), (w_out_pool, wop.at[pl.ds(0, G)]), (post_gain, post),
    ]
    copies = [pltpu.make_async_copy(src, dst, lsem.at[i]) for i, (src, dst) in enumerate(loads)]
    gw[16:128, :] = jnp.zeros((112, D), BF16)
    copies[0].start()
    for copy in tok_copies:
        copy.start()
    for copy in copies[1:]:
        copy.start()

    def norm_rows(i):
        tok_copies[i].wait()
        rows = pl.ds(256 * i, 256)
        total = jnp.zeros((256, 128), F32)
        for col in range(D // 128):
            piece = tok[rows, pl.ds(128 * col, 128)].astype(F32)
            total = total + piece * piece
        scale = lax.rsqrt(jnp.sum(total, axis=1, keepdims=True) / D + EPS)
        for col in range(D // 128):
            at = pl.ds(128 * col, 128)
            piece = tok[rows, at].astype(F32)
            nrm[rows, at] = (piece * scale * pre[:, at]).astype(BF16)

    copies[0].wait()
    norm_rows(0)
    for i in range(1, 5):
        copies[i].wait()
    for i in range(4):
        if i < 3:
            norm_rows(i + 1)
        rows = pl.ds(256 * i, 256)
        normed = nrm[rows, :]
        k[rows, :] = nn(normed, wk[...]).astype(BF16)
        v[rows, :] = nn(normed, wv[...]).astype(BF16)
        gz[rows, :] = nt(normed, gw[...])
    for i in range(5, 10):
        copies[i].wait()

    head8 = lax.broadcasted_iota(jnp.int32, (8, 128), 0) == tp
    lin, lfor = [], []
    for r in range(8):
        block = gz[pl.ds(128 * r, 128), :].T
        lin.append(jnp.sum(jnp.where(head8, block[0:8], 0.0), axis=0, keepdims=True))
        lfor.append(jnp.sum(jnp.where(head8, block[8:16], 0.0), axis=0, keepdims=True))
    own8 = lax.broadcasted_iota(jnp.int32, (1, 8), 1) == tp
    shift_i = jnp.sum(jnp.where(own8, bias_i[...], 0.0), axis=1, keepdims=True)
    shift_f = jnp.sum(jnp.where(own8, bias_f[...], 0.0), axis=1, keepdims=True)
    log_input = jnp.concatenate(lin, axis=0) + shift_i
    pre_keep = jnp.concatenate(lfor, axis=0) + shift_f
    log_keep = jnp.minimum(pre_keep, 0.0) - jnp.log1p(jnp.exp(-jnp.abs(pre_keep))) + fex[...]
    keep_run = scan_packed(log_keep, jnp.add, 0.0)
    offer = log_input - keep_run
    best = scan_packed(offer, jnp.maximum, NEG)
    keep_all = keep_run[7:8, 127:128]
    best_all = best[7:8, 127:128]
    write = jnp.exp(offer - best_all)
    colA = columns_of([write, best])

    def column(source, index, i):
        at = 8 * index + 2 * i
        return jnp.concatenate([source[:, at : at + 1], source[:, at + 1 : at + 2]], axis=0)

    state = jnp.zeros((H, H), F32)
    normal = jnp.zeros((1, H), F32)
    for i in range(4):
        rows = pl.ds(256 * i, 256)
        weighted = column(colA, 0, i) * k[rows, :].astype(F32)
        normal = normal + jnp.sum(weighted, axis=0, keepdims=True)
        state = state + tn(weighted.astype(BF16), v[rows, :])
    ustate[...] = state
    lane128 = lax.broadcasted_iota(jnp.int32, (1, 128), 1)
    bsend[0:1, :] = normal[:, 0:128]
    bsend[1:2, :] = normal[:, 128:256]
    bsend[2:3, :] = jnp.where(lane128 < 64, keep_all + best_all, keep_all)
    placed = jnp.concatenate([inn[...], jnp.zeros((1, 120), F32)], axis=1)
    bsend[3:4, :] = pltpu.roll(placed, 8 * lax.rem(sp, 16), 1)

    def pack_slab(j, carry):
        slab = ustate[pl.ds(pl.multiple_of(8 * j, 8), 8), :]
        usend[j] = jnp.concatenate([slab[:, 0:128], slab[:, 128:256]], axis=0).astype(BF16)
        return carry

    lax.fori_loop(0, NSP, pack_slab, 0)
    urecv[sp] = usend[sp]
    brecv[sp] = bsend[...]

    pl.semaphore_wait(barrier, NSP - 1 + NTP - 1)

    def b_copy(dst):
        return pltpu.make_async_remote_copy(
            src_ref=bsend, dst_ref=brecv.at[sp], send_sem=bsem.at[0], recv_sem=bsem.at[1],
            device_id={"sp": dst, "tp": tp}, device_id_type=MESH,
        )

    def u_copy(dst):
        return pltpu.make_async_remote_copy(
            src_ref=usend.at[dst], dst_ref=urecv.at[sp], send_sem=usem.at[0], recv_sem=usem.at[1],
            device_id={"sp": dst, "tp": tp}, device_id_type=MESH,
        )

    def s_copy(dst):
        return pltpu.make_async_remote_copy(
            src_ref=ssend.at[dst], dst_ref=srecv.at[sp], send_sem=ssem.at[0], recv_sem=ssem.at[1],
            device_id={"sp": dst, "tp": tp}, device_id_type=MESH,
        )

    def send_first(n, carry):
        dst = sp_peer(n)
        b_copy(dst).start()
        u_copy(dst).start()
        return carry

    def send_second(n, carry):
        s_copy(sp_peer(n)).start()
        return carry

    lax.fori_loop(0, NSP - 1, send_first, 0)
    w_copies = [
        pltpu.make_async_remote_copy(
            src_ref=src, dst_ref=dst, send_sem=wsend.at[i], recv_sem=wrecv.at[i], device_id=sib, device_id_type=MESH
        )
        for i, (src, dst) in enumerate([(w_out_memory, wom.at[pl.ds(H, H)]), (w_out_pool, wop.at[pl.ds(G, G)])])
    ]
    for copy in w_copies:
        copy.start()

    for i in range(10, 18):
        copies[i - 0].wait() if i < 17 else None
    for i in range(4):
        rows = pl.ds(256 * i, 256)
        both = nn(nrm[rows, :], wp[...])
        pool_ext[pl.ds(HALO + 256 * i, 256), :] = both[:, 0:G].astype(BF16)
        pgate[rows, :] = silu(both[:, G : 2 * G]) * pg[...]
    halo = pltpu.make_async_remote_copy(
        src_ref=pool_ext.at[pl.ds(T, HALO)], dst_ref=pool_ext.at[pl.ds(0, HALO)], send_sem=hsem.at[0],
        recv_sem=hsem.at[1], device_id={"sp": lax.rem(sp + 1, NSP), "tp": tp}, device_id_type=MESH,
    )
    halo.start()
    for i in range(4):
        rows = pl.ds(256 * i, 256)
        q[rows, :] = nn(nrm[rows, :], wq[...]).astype(BF16)

    head_scale = H ** (-0.5)
    for i in range(4):
        rows = pl.ds(256 * i, 256)
        length = 256 * (i + 1)
        scores = nt(q[rows, :], k[pl.ds(0, length), :])
        source = jnp.concatenate([offer[r : r + 1, :] for r in range(2 * (i + 1))], axis=1)
        exponent = source - column(colA, 1, i)
        ahead = lax.broadcasted_iota(jnp.int32, (256, length), 1) > lax.broadcasted_iota(
            jnp.int32, (256, length), 0
        ) + 256 * i
        weights = jnp.exp(jnp.where(ahead, NEG, exponent)) * scores * head_scale
        den[rows, :] = jnp.broadcast_to(jnp.sum(weights, axis=1, keepdims=True), (256, 128))
        num[rows, :] = nn(weights.astype(BF16), v[pl.ds(0, length), :])
    for i in range(4):
        rows = pl.ds(256 * i, 256)
        gate[rows, :] = silu(nn(nrm[rows, :], wg[...])) * mg[...]

    pltpu.make_async_copy(brecv.at[pl.ds(0, NSP - 1)], brecv.at[pl.ds(0, NSP - 1)], bsem.at[1]).wait()
    pltpu.make_async_copy(urecv.at[pl.ds(0, NSP - 1)], urecv.at[pl.ds(0, NSP - 1)], usem.at[1]).wait()
    memory = jnp.concatenate([im[:, 0:128], im[:, 128:256]], axis=0)
    start_low = jnp.zeros((1, 128), F32)
    start_high = jnp.zeros((1, 128), F32)
    for j in range(16):
        start_low = start_low + brecv[j, 3:4, :]
        start_high = start_high + brecv[16 + j, 3:4, :]
    carried_n = jnp.concatenate([start_low, start_high], axis=0)
    stab = jnp.zeros((1, 1), F32)
    my_stab = jnp.zeros((1, 1), F32)
    my_n = carried_n
    for j in range(NSP):
        mine = sp == j
        my_stab = jnp.where(mine, stab, my_stab)
        my_n = jnp.where(mine, carried_n, my_n)
        ssend[j] = memory.astype(BF16)
        if j < NSP - 1:
            piece_stab = brecv[j, 2:3, 0:1]
            piece_keep = brecv[j, 2:3, 64:65]
            new_stab = jnp.maximum(stab + piece_keep, piece_stab)
            fade = jnp.exp(stab + piece_keep - new_stab)
            weight = jnp.exp(piece_stab - new_stab)
            memory = fade * memory + weight * urecv[j].astype(F32)
            carried_n = fade * carried_n + weight * brecv[j, 0:2, :]
            stab = new_stab
    srecv[sp] = ssend[sp]
    lax.fori_loop(0, NSP - 1, send_second, 0)

    joint = jnp.maximum(best, my_stab)
    local_weight = jnp.exp(best - joint)
    carry_weight = jnp.exp(my_stab - joint) * head_scale
    least = jnp.exp(-(keep_run + joint))
    cols[...] = columns_of([local_weight, carry_weight, least])
    n_row = jnp.concatenate([my_n[0:1, :], my_n[1:2, :]], axis=1)
    colB = cols[...]
    for i in range(4):
        rows = pl.ds(256 * i, 256)
        carried = jnp.sum(q[rows, :].astype(F32) * n_row, axis=1, keepdims=True)
        full = den[rows, 0:1] * column(colB, 0, i) + column(colB, 1, i) * carried
        inverse = 1.0 / jnp.maximum(jnp.abs(full), column(colB, 2, i))
        num[rows, :] = num[rows, :] * (column(colB, 0, i) * inverse)
        den[rows, :] = jnp.broadcast_to(column(colB, 1, i) * inverse, (256, 128))

    halo.wait_recv()
    first = jnp.where(sp == 0, 0.0, 1.0)
    pool_ext[pl.ds(0, HALO), :] = (pool_ext[pl.ds(0, HALO), :].astype(F32) * first).astype(BF16)
    window = lax.shift_left(jnp.int32(2), tp)
    for i in range(4):
        rows = pl.ds(256 * i, 256)
        near = pool_ext[pl.ds(256 * i, 512), :]
        target = lax.broadcasted_iota(jnp.int32, (256, 512), 0) + HALO
        back = target - lax.broadcasted_iota(jnp.int32, (256, 512), 1)
        band = jnp.where((back >= 0) & (back < window), 1.0, 0.0).astype(BF16)
        sums = nn(band, near)
        place = sp * T + 256 * i + lax.broadcasted_iota(jnp.int32, (256, 1), 0) + 1
        count = jnp.minimum(place, window).astype(F32)
        pooled = (sums / count - near[HALO:, :].astype(F32)).astype(BF16)
        mixed = nn(pooled, pm[...]) * pgate[rows, :]
        zbuf[2 * i, :, H : H + G] = mixed[0:128].astype(BF16)
        zbuf[2 * i + 1, :, H : H + G] = mixed[128:256].astype(BF16)
    for i in range(17, 20):
        copies[i].wait()

    pltpu.make_async_copy(srecv.at[pl.ds(0, NSP - 1)], srecv.at[pl.ds(0, NSP - 1)], ssem.at[1]).wait()
    for j in range(NSP):
        slab = srecv[j].astype(F32)
        smat[8 * j : 8 * j + 8, 0:128] = slab[0:8]
        smat[8 * j : 8 * j + 8, 128:256] = slab[8:16]
    held = smat[...].astype(BF16)
    lane_sq = lax.broadcasted_iota(jnp.int32, (128, 128), 1)
    squares = jnp.zeros((128, 128), F32)
    for i in range(4):
        rows = pl.ds(256 * i, 256)
        memory_rows = num[rows, :] + den[rows, 0:1] * nn(q[rows, :], held)
        sq = jnp.sum(memory_rows * memory_rows, axis=1, keepdims=True)
        squares = jnp.where(lane_sq == 2 * i, sq[0:128], squares)
        squares = jnp.where(lane_sq == 2 * i + 1, sq[128:256], squares)
        gated = (memory_rows * gate[rows, :]).astype(BF16)
        zbuf[2 * i, :, 0:H] = gated[0:128]
        zbuf[2 * i + 1, :, 0:H] = gated[128:256]
    own_sq = squares.T[0:8]
    sqs[...] = own_sq

    def sq_copy(n):
        return pltpu.make_async_remote_copy(
            src_ref=sqs, dst_ref=sqr.at[n], send_sem=qsem.at[0], recv_sem=qsem.at[1],
            device_id={"sp": sp, "tp": lax.rem(tp + n + 1, NTP)}, device_id_type=MESH,
        )

    def z_copy(n):
        return pltpu.make_async_remote_copy(
            src_ref=zbuf.at[2 * n + 1 - c], dst_ref=zsib.at[n], send_sem=zsem.at[0], recv_sem=zsem.at[1],
            device_id=sib, device_id_type=MESH,
        )

    for n in range(NTP - 1):
        sq_copy(n).start()
    for n in range(NY):
        z_copy(n).start()
    for copy in w_copies:
        copy.wait_recv()
    pltpu.make_async_copy(zsib, zsib, zsem.at[1]).wait()
    pltpu.make_async_copy(sqr, sqr, qsem.at[1]).wait()
    total = own_sq
    for n in range(NTP - 1):
        total = total + sqr[n]
    sqs_scale = lax.rsqrt(total / (NTP * H) + EPS)
    cols[0:8, :] = sqs_scale
    eye = lax.broadcasted_iota(jnp.int32, (128, 128), 0) == lax.broadcasted_iota(jnp.int32, (128, 128), 1)

    def out_block(dy):
        to = lax.rem(y + dy, NY)
        mine, other = zbuf[2 * to + c], zsib[to]
        row = cols[pl.ds(2 * to + c, 1), :]
        scale = jnp.sum(jnp.where(eye, jnp.broadcast_to(row, (128, 128)), 0.0), axis=1, keepdims=True)
        memory_in = jnp.concatenate([mine[:, 0:H], other[:, 0:H]], axis=1)
        pool_in = jnp.concatenate([mine[:, H:], other[:, H:]], axis=1)
        for half in range(2):
            for quarter in range(2):
                at = pl.ds(1024 * half + 512 * quarter, 512)
                term = nn(memory_in, wom[:, at]) * scale + nn(pool_in, wop[:, at])
                part[dy, half, :, pl.ds(512 * quarter, 512)] = term.astype(BF16)

    def rs_copy(n, src, dst, to):
        return pltpu.make_async_remote_copy(
            src_ref=src, dst_ref=dst, send_sem=rsend.at[n], recv_sem=rrecv.at[n], device_id=to, device_id_type=MESH
        )

    rs = [
        rs_copy(0, part.at[2, 0], r1, up), rs_copy(1, part.at[2, 1], r2, down),
        rs_copy(2, part.at[1, 1], r3, up), rs_copy(3, part.at[3, 0], r4, down),
        rs_copy(4, fwd.at[0], r5, up), rs_copy(5, fwd.at[1], r6, down),
    ]
    out_block(2)
    rs[0].start()
    rs[1].start()
    out_block(1)
    rs[2].start()
    out_block(3)
    rs[3].start()
    out_block(0)
    rs[0].wait_recv()
    fwd[0] = (part[1, 0].astype(F32) + r1[...].astype(F32)).astype(BF16)
    rs[4].start()
    rs[1].wait_recv()
    fwd[1] = (part[3, 1].astype(F32) + r2[...].astype(F32)).astype(BF16)
    rs[5].start()
    for n in range(2, 6):
        rs[n].wait_recv()
    low = part[0, 0].astype(F32) + r4[...].astype(F32) + r5[...].astype(F32)
    high = part[0, 1].astype(F32) + r3[...].astype(F32) + r6[...].astype(F32)
    mean = (jnp.sum(low * low, axis=1, keepdims=True) + jnp.sum(high * high, axis=1, keepdims=True)) / D
    scale = lax.rsqrt(mean + EPS)
    obuf[:, 0:1024] = (low * scale * post[:, 0:1024]).astype(BF16)
    obuf[:, 1024:2048] = (high * scale * post[:, 1024:2048]).astype(BF16)
    finish = pltpu.make_async_copy(obuf, out, osem.at[0])
    finish.start()

    def drain_first(n, carry):
        b_copy(sp_peer(n)).wait_send()
        u_copy(sp_peer(n)).wait_send()
        s_copy(sp_peer(n)).wait_send()
        return carry

    lax.fori_loop(0, NSP - 1, drain_first, 0)
    for copy in w_copies:
        copy.wait_send()
    halo.wait_send()
    for n in range(NTP - 1):
        sq_copy(n).wait_send()
    for n in range(NY):
        z_copy(n).wait_send()
    for copy in rs:
        copy.wait_send()
    finish.wait()


def body(
    tokens, pre_gain, w_query, w_key, w_value, memory_output_gate_weight, w_input_gate, w_forget_gate, input_bias,
    forget_bias, forget_extra, initial_memory, initial_normal, memory_gain, w_pool_input, w_pool_gate, pool_mix,
    pool_gain, w_out_memory, w_out_pool, post_gain,
):
    args = (
        tokens, pre_gain.reshape(1, D), w_query, w_key, w_value, memory_output_gate_weight, w_input_gate.T,
        w_forget_gate.T, input_bias.reshape(1, 8), forget_bias.reshape(1, 8), forget_extra.reshape(8, 128),
        initial_memory.reshape(8, H), initial_normal, memory_gain.reshape(1, D), w_pool_input, w_pool_gate, pool_mix,
        pool_gain.reshape(1, NTP * G), w_out_memory, w_out_pool, post_gain.reshape(1, D),
    )
    vmem = pltpu.VMEM
    dma = pltpu.SemaphoreType.DMA
    scratch = [
        vmem((T, D), BF16), vmem((T, D), BF16), vmem((D, H), BF16), vmem((D, H), BF16), vmem((D, H), BF16),
        vmem((D, H), BF16), vmem((D, 2 * G), BF16), vmem((128, D), BF16), vmem((1, D), F32), vmem((1, 8), F32),
        vmem((1, 8), F32), vmem((8, 128), F32), vmem((8, H), F32), vmem((1, 8), F32), vmem((1, H), F32),
        vmem((G, G), BF16), vmem((1, G), F32), vmem((2 * H, D), BF16), vmem((2 * G, D), BF16), vmem((1, D), F32),
        vmem((T, 128), F32), vmem((T, H), BF16), vmem((T, H), BF16), vmem((T, H), BF16), vmem((T, H), F32),
        vmem((HALO + T, G), BF16), vmem((T, G), F32), vmem((T, H), F32), vmem((T, 128), F32), vmem((128, 128), F32),
        vmem((H, H), F32), vmem((NSP, 16, 128), BF16), vmem((NSP, 16, 128), BF16), vmem((4, 128), F32),
        vmem((NSP, 4, 128), F32), vmem((NSP, 16, 128), BF16), vmem((NSP, 16, 128), BF16), vmem((H, H), F32),
        vmem((8, 128), F32), vmem((NTP - 1, 8, 128), F32), vmem((NTP, 128, H + G), BF16), vmem((NY, 128, H + G), BF16),
        vmem((NY, 2, 128, 1024), BF16), vmem((2, 128, 1024), BF16), vmem((128, 1024), BF16), vmem((128, 1024), BF16),
        vmem((128, 1024), BF16), vmem((128, 1024), BF16), vmem((128, 1024), BF16), vmem((128, 1024), BF16),
        vmem((128, D), BF16),
        dma((20,)), dma((4,)), dma((1,)), dma((2,)), dma((2,)), dma((2,)), dma((2,)), dma((2,)), dma((2,)), dma((2,)),
        dma((2,)), dma((6,)), dma((6,)),
    ]
    anywhere = pl.BlockSpec(memory_space=pl.ANY)
    return pl.pallas_call(
        kernel,
        out_shape=jax.ShapeDtypeStruct((128, D), BF16),
        in_specs=[anywhere] * len(args),
        out_specs=anywhere,
        scratch_shapes=scratch,
        compiler_params=pltpu.CompilerParams(
            collective_id=0, has_side_effects=True, vmem_limit_bytes=60 * 1024 * 1024
        ),
    )(*args)


def solution(mesh):
    in_specs = (
        P("sp", None), P(), P(None, "tp"), P(None, "tp"), P(None, "tp"), P(None, "tp"), P(), P(), P(), P(),
        P("sp", "tp"), P("tp", "sp", None), P("tp", "sp"), P(), P(None, "tp"), P(None, "tp"), P(), P(),
        P("tp", None), P("tp", None), P(),
    )
    return jax.shard_map(
        body, mesh=mesh, in_specs=in_specs, out_specs=P(("sp", "tp"), None), check_vma=False
    )
```

```python
import jax
import jax.numpy as jnp
from jax import lax
from jax.experimental import pallas as pl
from jax.experimental.pallas import tpu as pltpu
from jax.sharding import PartitionSpec as P

EPS = 1e-6
NEG = -1e30
F32 = jnp.float32
BF16 = jnp.bfloat16
MESH = pl.DeviceIdType.MESH

T = 1024
D = 2048
H = 256
G = 128
NSP = 32
NZ, NX = 8, 4
NTP = 8
NY = 4
HALF = NSP // 2
HALO = 256


def nn(a, b):
    return jnp.dot(a, b, preferred_element_type=F32)


def nt(a, b):
    return lax.dot_general(a, b, (((1,), (1,)), ((), ())), preferred_element_type=F32)


def tn(a, b):
    return lax.dot_general(a, b, (((0,), (0,)), ((), ())), preferred_element_type=F32)


def silu(x):
    return x / (1.0 + jnp.exp(-x))


class Phases:
    scope = None

    def __call__(self, name):
        if self.scope is not None:
            self.scope.__exit__(None, None, None)
        self.scope = jax.named_scope(name) if name else None
        if name:
            self.scope.__enter__()


def scan_packed(x, combine, fill):
    lane = lax.broadcasted_iota(jnp.int32, (8, 128), 1)
    sub = lax.broadcasted_iota(jnp.int32, (8, 128), 0)
    for step in (1, 2, 4, 8, 16, 32, 64):
        x = combine(x, jnp.where(lane >= step, pltpu.roll(x, step, 1), fill))
    rows = jnp.broadcast_to(x[:, 127:128], (8, 128))
    before = jnp.where(sub >= 1, pltpu.roll(rows, 1, 0), fill)
    for step in (1, 2, 4):
        before = combine(before, jnp.where(sub >= step, pltpu.roll(before, step, 0), fill))
    return combine(x, before)


def columns_of(packed):
    rows = jnp.concatenate(packed + [jnp.zeros((128 - 8 * len(packed), 128), F32)], axis=0)
    return rows.T


def kernel(
    tokens, pre_gain, w_query, w_key, w_value, w_gate, w_in, w_forget, in_bias, forget_bias, extra, init_memory,
    init_normal, memory_gain, w_pool_in, w_pool_gate, pool_mix, pool_gain, w_out_memory, w_out_pool, post_gain,
    out,
    tok, nrm, wq, wk, wv, wg, wp, wpg, gw, pre, bias_i, bias_f, fex, im, inn, mg, pm, pg, wom, wop, post,
    gz, q, k, v, gate, pool_ext, pgate, num, den, cols,
    ustate, usend, urecv, bsend, brecv, ssend, srecv, smat,
    sqs, sqr, zbuf, zsib, pbuf, psib, ppart, part, fwd, r1, r2, r3, r4, r5, r6, rp1, rp2,
    lsem, tsem, wsend, wrecv, usem, bsem, hsem, ssem, qsem, zsem, psem, rsend, rrecv,
):
    sp = lax.axis_index("sp")
    tp = lax.axis_index("tp")
    z, x = sp // NX, sp % NX
    y, c = tp // 2, tp % 2
    sib = {"sp": sp, "tp": 2 * y + (1 - c)}
    up = {"sp": sp, "tp": 2 * lax.rem(y + 1, NY) + c}
    down = {"sp": sp, "tp": 2 * lax.rem(y + NY - 1, NY) + c}

    def sp_peer(n):
        kz = n // NX
        dz = lax.rem(4 + (kz + 1) // 2 * (1 - 2 * lax.rem(kz, 2)) + NZ, NZ)
        dx = lax.rem(2 + lax.rem(n, NX), NX)
        dx = jnp.where(lax.rem(n, NX) == 1, 1, jnp.where(lax.rem(n, NX) == 2, 3, jnp.where(lax.rem(n, NX) == 3, 0, 2)))
        return lax.rem(z + dz, NZ) * NX + lax.rem(x + dx, NX)

    phase = Phases()
    phase("loads")
    tok_copies = [
        pltpu.make_async_copy(tokens.at[pl.ds(256 * i, 256)], tok.at[pl.ds(256 * i, 256)], tsem.at[i]) for i in range(4)
    ]
    loads = [
        (pre_gain, pre), (w_in, gw.at[pl.ds(0, 8)]), (w_forget, gw.at[pl.ds(8, 8)]), (w_key, wk),
        (w_pool_in, wp.at[:, pl.ds(0, G)]), (w_value, wv),
        (in_bias, bias_i), (forget_bias, bias_f), (extra, fex), (init_memory, im), (init_normal, inn),
        (w_query, wq), (w_gate, wg), (w_pool_gate, wpg),
        (memory_gain.at[:, pl.ds(pl.multiple_of(tp * H, H), H)], mg), (pool_mix.at[tp], pm),
        (pool_gain.at[:, pl.ds(pl.multiple_of(tp * G, G), G)], pg),
        (w_out_memory, wom.at[pl.ds(0, H)]), (w_out_pool, wop.at[pl.ds(0, G)]), (post_gain, post),
    ]
    copies = [pltpu.make_async_copy(src, dst, lsem.at[i]) for i, (src, dst) in enumerate(loads)]
    tok_copies[0].start()
    for copy in copies[0:3]:
        copy.start()
    tok_copies[1].start()
    copies[3].start()
    copies[4].start()
    tok_copies[2].start()
    tok_copies[3].start()

    phase("greet")
    barrier = pltpu.get_barrier_semaphore()

    def greet_sp(n, carry):
        pl.semaphore_signal(barrier, inc=1, device_id={"sp": sp_peer(n), "tp": tp}, device_id_type=MESH)
        return carry

    def greet_tp(n, carry):
        pl.semaphore_signal(barrier, inc=1, device_id={"sp": sp, "tp": lax.rem(tp + n, NTP)}, device_id_type=MESH)
        return carry

    lax.fori_loop(0, NSP - 1, greet_sp, 0)
    lax.fori_loop(1, NTP, greet_tp, 0)

    def norm_rows(i):
        tok_copies[i].wait()
        rows = pl.ds(256 * i, 256)
        total = jnp.zeros((256, 128), F32)
        for col in range(D // 128):
            piece = tok[rows, pl.ds(128 * col, 128)].astype(F32)
            total = total + piece * piece
        scale = lax.rsqrt(jnp.sum(total, axis=1, keepdims=True) / D + EPS)
        for col in range(D // 128):
            at = pl.ds(128 * col, 128)
            piece = tok[rows, at].astype(F32)
            nrm[rows, at] = (piece * scale * pre[:, at]).astype(BF16)

    phase("gw")
    for i in (0, 1, 2):
        copies[i].wait()
    for col in range(D // 128):
        at = pl.ds(128 * col, 128)
        logits = jnp.concatenate([gw[:, at].astype(F32), jnp.zeros((112, 128), F32)], axis=0)
        wp[at, G : 2 * G] = logits.T.astype(BF16)
    phase("norm0")
    norm_rows(0)
    for copy in copies[5:]:
        copy.start()
    for i in (3, 4):
        copies[i].wait()
    for i in range(4):
        phase("kv%d" % i)
        if i < 3:
            norm_rows(i + 1)
        rows = pl.ds(256 * i, 256)
        normed = nrm[rows, :]
        both = nn(normed, wp[...])
        pool_ext[pl.ds(HALO + 256 * i, 256), :] = both[:, 0:G].astype(BF16)
        gz[rows, :] = both[:, G : 2 * G]
        k[rows, :] = nn(normed, wk[...]).astype(BF16)
    phase("gates")
    for i in range(5, 11):
        copies[i].wait()
    for i in range(2):
        rows = pl.ds(512 * i, 512)
        v[rows, :] = nn(nrm[rows, :], wv[...]).astype(BF16)

    head8 = lax.broadcasted_iota(jnp.int32, (8, 128), 0) == tp
    lin, lfor = [], []
    for r in range(8):
        block = gz[pl.ds(128 * r, 128), :].T
        lin.append(jnp.sum(jnp.where(head8, block[0:8], 0.0), axis=0, keepdims=True))
        lfor.append(jnp.sum(jnp.where(head8, block[8:16], 0.0), axis=0, keepdims=True))
    own8 = lax.broadcasted_iota(jnp.int32, (1, 8), 1) == tp
    shift_i = jnp.sum(jnp.where(own8, bias_i[...], 0.0), axis=1, keepdims=True)
    shift_f = jnp.sum(jnp.where(own8, bias_f[...], 0.0), axis=1, keepdims=True)
    log_input = jnp.concatenate(lin, axis=0) + shift_i
    pre_keep = jnp.concatenate(lfor, axis=0) + shift_f
    log_keep = jnp.minimum(pre_keep, 0.0) - jnp.log1p(jnp.exp(-jnp.abs(pre_keep))) + fex[...]
    keep_run = scan_packed(log_keep, jnp.add, 0.0)
    offer = log_input - keep_run
    best = scan_packed(offer, jnp.maximum, NEG)
    keep_all = keep_run[7:8, 127:128]
    best_all = best[7:8, 127:128]
    write = jnp.exp(offer - best_all)
    colA = columns_of([write, best])

    def column(source, index, i):
        at = 8 * index + 2 * i
        return jnp.concatenate([source[:, at : at + 1], source[:, at + 1 : at + 2]], axis=0)

    phase("state")
    state = jnp.zeros((H, H), F32)
    normal = jnp.zeros((1, H), F32)
    for i in range(4):
        rows = pl.ds(256 * i, 256)
        weighted = column(colA, 0, i) * k[rows, :].astype(F32)
        normal = normal + jnp.sum(weighted, axis=0, keepdims=True)
        state = state + tn(weighted.astype(BF16), v[rows, :])
    ustate[...] = state
    lane128 = lax.broadcasted_iota(jnp.int32, (1, 128), 1)
    bsend[0:1, :] = normal[:, 0:128]
    bsend[1:2, :] = normal[:, 128:256]
    bsend[2:3, :] = jnp.where(lane128 < 64, keep_all + best_all, keep_all)
    placed = jnp.concatenate([inn[...], jnp.zeros((1, 120), F32)], axis=1)
    bsend[3:4, :] = pltpu.roll(placed, 8 * lax.rem(sp, 16), 1)

    phase("pack")
    def pack_slab(j, carry):
        slab = ustate[pl.ds(pl.multiple_of(8 * j, 8), 8), :]
        usend[j] = jnp.concatenate([slab[:, 0:128], slab[:, 128:256]], axis=0).astype(BF16)
        return carry

    lax.fori_loop(0, NSP, pack_slab, 0)
    urecv[sp] = usend[sp]
    brecv[sp] = bsend[...]

    phase("barrier")
    pl.semaphore_wait(barrier, NSP - 1 + NTP - 1)

    def b_copy(dst):
        return pltpu.make_async_remote_copy(
            src_ref=bsend, dst_ref=brecv.at[sp], send_sem=bsem.at[0], recv_sem=bsem.at[1 + sp // HALF],
            device_id={"sp": dst, "tp": tp}, device_id_type=MESH,
        )

    def u_copy(dst):
        return pltpu.make_async_remote_copy(
            src_ref=usend.at[dst], dst_ref=urecv.at[sp], send_sem=usem.at[0], recv_sem=usem.at[1 + sp // HALF],
            device_id={"sp": dst, "tp": tp}, device_id_type=MESH,
        )

    def s_copy(dst):
        return pltpu.make_async_remote_copy(
            src_ref=ssend.at[dst], dst_ref=srecv.at[sp], send_sem=ssem.at[0], recv_sem=ssem.at[1],
            device_id={"sp": dst, "tp": tp}, device_id_type=MESH,
        )

    def send_first(n, carry):
        dst = sp_peer(n)
        b_copy(dst).start()
        u_copy(dst).start()
        return carry

    def send_second(half):
        def send(n, carry):
            dst = HALF * half + lax.rem(sp + HALF // 2 + n, HALF)

            @pl.when(dst != sp)
            def _():
                s_copy(dst).start()

            return carry

        lax.fori_loop(0, HALF, send, 0)

    def wait_first(half):
        def wait(count):
            pltpu.make_async_copy(brecv.at[pl.ds(0, count)], brecv.at[pl.ds(0, count)], bsem.at[1 + half]).wait()
            pltpu.make_async_copy(urecv.at[pl.ds(0, count)], urecv.at[pl.ds(0, count)], usem.at[1 + half]).wait()

        @pl.when(sp // HALF == half)
        def _():
            wait(HALF - 1)

        @pl.when(sp // HALF != half)
        def _():
            wait(HALF)

    phase("send1")
    lax.fori_loop(0, NSP - 1, send_first, 0)
    w_copies = [
        pltpu.make_async_remote_copy(
            src_ref=src, dst_ref=dst, send_sem=wsend.at[i], recv_sem=wrecv.at[i], device_id=sib, device_id_type=MESH
        )
        for i, (src, dst) in enumerate([(w_out_memory, wom.at[pl.ds(H, H)]), (w_out_pool, wop.at[pl.ds(G, G)])])
    ]
    for copy in w_copies:
        copy.start()

    halo = pltpu.make_async_remote_copy(
        src_ref=pool_ext.at[pl.ds(T, HALO)], dst_ref=pool_ext.at[pl.ds(0, HALO)], send_sem=hsem.at[0],
        recv_sem=hsem.at[1], device_id={"sp": lax.rem(sp + 1, NSP), "tp": tp}, device_id_type=MESH,
    )

    @pl.when(sp < NSP - 1)
    def _():
        halo.start()

    phase("pgate")
    for i in range(11, 17):
        copies[i].wait()
    for i in range(2):
        rows = pl.ds(512 * i, 512)
        pgate[rows, :] = silu(nn(nrm[rows, :], wpg[...])) * pg[...]

    def p_copy(n):
        return pltpu.make_async_remote_copy(
            src_ref=pbuf.at[2 * n + 1 - c], dst_ref=psib.at[n], send_sem=psem.at[0], recv_sem=psem.at[1],
            device_id=sib, device_id_type=MESH,
        )

    order = (2, 1, 3, 0)

    def rs_copy(n, src, dst, to):
        return pltpu.make_async_remote_copy(
            src_ref=src, dst_ref=dst, send_sem=rsend.at[n], recv_sem=rrecv.at[n], device_id=to, device_id_type=MESH
        )

    rs = [
        rs_copy(0, part.at[2, 0], r1, up), rs_copy(1, part.at[2, 1], r2, down),
        rs_copy(2, part.at[1, 1], r3, up), rs_copy(3, part.at[3, 0], r4, down),
        rs_copy(4, fwd.at[0], r5, up), rs_copy(5, fwd.at[1], r6, down),
        rs_copy(6, ppart.at[0], rp1, up), rs_copy(7, ppart.at[1], rp2, down),
    ]

    def memory_inputs(dy):
        to = lax.rem(y + dy, NY)
        return jnp.concatenate([zbuf[2 * to + c], zsib[to]], axis=1)

    def pool_inputs(dy):
        to = lax.rem(y + dy, NY)
        return jnp.concatenate([pbuf[2 * to + c], psib[to]], axis=1)

    phase("q")
    for i in range(2):
        rows = pl.ds(512 * i, 512)
        q[rows, :] = nn(nrm[rows, :], wq[...]).astype(BF16)

    memory = jnp.concatenate([im[:, 0:128], im[:, 128:256]], axis=0)
    stab = jnp.zeros((1, 1), F32)
    my_stab = jnp.zeros((1, 1), F32)
    carried_n = jnp.zeros((2, 128), F32)
    my_n = carried_n
    fade_all = jnp.ones((1, 1), F32)
    my_fade = fade_all
    for half in range(2):
        phase("wait1_%d" % half)
        wait_first(half)
        phase("scan%d" % half)
        for j in range(HALF * half, HALF * half + HALF):
            mine = sp == j
            my_stab = jnp.where(mine, stab, my_stab)
            my_n = jnp.where(mine, carried_n, my_n)
            my_fade = jnp.where(mine, fade_all, my_fade)
            ssend[j] = memory.astype(BF16)
            piece_stab = brecv[j, 2:3, 0:1]
            piece_keep = brecv[j, 2:3, 64:65]
            new_stab = jnp.maximum(stab + piece_keep, piece_stab)
            fade = jnp.exp(stab + piece_keep - new_stab)
            weight = jnp.exp(piece_stab - new_stab)
            memory = fade * memory + weight * urecv[j].astype(F32)
            carried_n = fade * carried_n + weight * brecv[j, 0:2, :]
            fade_all = fade_all * fade
            stab = new_stab

        phase("send2_%d" % half)

        @pl.when(sp // HALF == half)
        def _():
            srecv[sp] = ssend[sp]

        send_second(half)
        if half == 0:
            phase("pool")
            @pl.when(sp > 0)
            def _():
                halo.wait_recv()

            @pl.when(sp == 0)
            def _():
                pool_ext[pl.ds(0, HALO), :] = jnp.zeros((HALO, G), BF16)

            window = lax.shift_left(jnp.int32(2), tp)
            for i in range(4):
                rows = pl.ds(256 * i, 256)
                near = pool_ext[pl.ds(256 * i, 512), :]
                target = lax.broadcasted_iota(jnp.int32, (256, 512), 0) + HALO
                back = target - lax.broadcasted_iota(jnp.int32, (256, 512), 1)
                band = jnp.where((back >= 0) & (back < window), 1.0, 0.0).astype(BF16)
                sums = nn(band, near)
                place = sp * T + 256 * i + lax.broadcasted_iota(jnp.int32, (256, 1), 0) + 1
                count = jnp.minimum(place, window).astype(F32)
                pooled = (sums / count - near[HALO:, :].astype(F32)).astype(BF16)
                mixed = nn(pooled, pm[...]) * pgate[rows, :]
                pbuf[2 * i] = mixed[0:128].astype(BF16)
                pbuf[2 * i + 1] = mixed[128:256].astype(BF16)

            for n in range(NY):
                p_copy(n).start()

            phase("attn")
            head_scale = H ** (-0.5)
            for i in range(4):
                rows = pl.ds(256 * i, 256)
                length = 256 * (i + 1)
                scores = nt(q[rows, :], k[pl.ds(0, length), :])
                source = jnp.concatenate([offer[r : r + 1, :] for r in range(2 * (i + 1))], axis=1)
                exponent = source - column(colA, 1, i)
                ahead = lax.broadcasted_iota(jnp.int32, (256, length), 1) > lax.broadcasted_iota(
                    jnp.int32, (256, length), 0
                ) + 256 * i
                weights = jnp.exp(jnp.where(ahead, NEG, exponent)) * scores * head_scale
                den[rows, :] = jnp.broadcast_to(jnp.sum(weights, axis=1, keepdims=True), (256, 128))
                num[rows, :] = nn(weights.astype(BF16), v[pl.ds(0, length), :])

    phase("pout")
    for i in range(17, 20):
        copies[i].wait()
    for copy in w_copies:
        copy.wait_recv()
    pltpu.make_async_copy(psib, psib, psem.at[1]).wait()
    pool_in = pool_inputs(2)
    for quarter in range(4):
        at = pl.ds(512 * (quarter % 2), 512)
        ppart[quarter // 2, :, at] = nn(pool_in, wop[:, pl.ds(512 * quarter, 512)]).astype(BF16)
    rs[6].start()
    rs[7].start()

    start_low = jnp.zeros((1, 128), F32)
    start_high = jnp.zeros((1, 128), F32)
    for j in range(HALF):
        start_low = start_low + brecv[j, 3:4, :]
        start_high = start_high + brecv[HALF + j, 3:4, :]
    my_n = my_n + my_fade * jnp.concatenate([start_low, start_high], axis=0)

    phase("gate")
    for i in range(2):
        rows = pl.ds(512 * i, 512)
        gate[rows, :] = silu(nn(nrm[rows, :], wg[...])) * mg[...]

    phase("denom")
    joint = jnp.maximum(best, my_stab)
    local_weight = jnp.exp(best - joint)
    carry_weight = jnp.exp(my_stab - joint) * head_scale
    least = jnp.exp(-(keep_run + joint))
    cols[...] = columns_of([local_weight, carry_weight, least])
    n_row = jnp.concatenate([my_n[0:1, :], my_n[1:2, :]], axis=1)
    colB = cols[...]
    for i in range(4):
        rows = pl.ds(256 * i, 256)
        carried = jnp.sum(q[rows, :].astype(F32) * n_row, axis=1, keepdims=True)
        full = den[rows, 0:1] * column(colB, 0, i) + column(colB, 1, i) * carried
        inverse = 1.0 / jnp.maximum(jnp.abs(full), column(colB, 2, i))
        num[rows, :] = num[rows, :] * (column(colB, 0, i) * inverse)
        den[rows, :] = jnp.broadcast_to(column(colB, 1, i) * inverse, (256, 128))

    phase("wait2")
    pltpu.make_async_copy(srecv.at[pl.ds(0, NSP - 1)], srecv.at[pl.ds(0, NSP - 1)], ssem.at[1]).wait()
    phase("finish")
    for j in range(NSP):
        slab = srecv[j].astype(F32)
        smat[8 * j : 8 * j + 8, 0:128] = slab[0:8]
        smat[8 * j : 8 * j + 8, 128:256] = slab[8:16]
    held = smat[...].astype(BF16)
    lane_sq = lax.broadcasted_iota(jnp.int32, (128, 128), 1)
    squares = jnp.zeros((128, 128), F32)

    def z_copy(n):
        to = lax.rem(y + order[n], NY)
        return pltpu.make_async_remote_copy(
            src_ref=zbuf.at[2 * to + 1 - c], dst_ref=zsib.at[to], send_sem=zsem.at[n], recv_sem=zsem.at[NY + n],
            device_id=sib, device_id_type=MESH,
        )

    z_copies = [z_copy(n) for n in range(NY)]
    for n in range(NY):
        for core in (1 - c, c):
            block = 2 * lax.rem(y + order[n], NY) + core
            rows = pl.ds(pl.multiple_of(128 * block, 128), 128)
            memory_rows = num[rows, :] + den[rows, 0:1] * nn(q[rows, :], held)
            sq = jnp.sum(memory_rows * memory_rows, axis=1, keepdims=True)
            squares = jnp.where(lane_sq == block, sq, squares)
            zbuf[block] = (memory_rows * gate[rows, :]).astype(BF16)
        z_copies[n].start()
    own_sq = squares.T[0:8]
    sqs[...] = own_sq

    def sq_copy(n):
        return pltpu.make_async_remote_copy(
            src_ref=sqs, dst_ref=sqr.at[n], send_sem=qsem.at[0], recv_sem=qsem.at[1],
            device_id={"sp": sp, "tp": lax.rem(tp + n + 1, NTP)}, device_id_type=MESH,
        )

    for n in range(NTP - 1):
        sq_copy(n).start()
    eye = lax.broadcasted_iota(jnp.int32, (128, 128), 0) == lax.broadcasted_iota(jnp.int32, (128, 128), 1)

    def out_scale(dy):
        to = lax.rem(y + dy, NY)
        row = cols[pl.ds(2 * to + c, 1), :]
        return jnp.sum(jnp.where(eye, jnp.broadcast_to(row, (128, 128)), 0.0), axis=1, keepdims=True)

    phase("zwait")
    z_copies[0].wait_recv()
    phase("ob2")
    memory_in = memory_inputs(2)
    for half in range(2):
        for quarter in range(2):
            at = pl.ds(512 * quarter, 512)
            part[2, half, :, at] = nn(memory_in, wom[:, pl.ds(1024 * half + 512 * quarter, 512)]).astype(BF16)
        rs[half].start()

    phase("sqwait")
    pltpu.make_async_copy(sqr, sqr, qsem.at[1]).wait()
    phase("scale")
    total = own_sq
    for n in range(NTP - 1):
        total = total + sqr[n]
    cols[0:8, :] = lax.rsqrt(total / (NTP * H) + EPS)
    for n, dy in ((1, 1), (2, 3), (3, 0)):
        phase("ob%d" % dy)
        z_copies[n].wait_recv()
        memory_in, pool_in = memory_inputs(dy), pool_inputs(dy)
        scale = out_scale(dy)
        for half in (1, 0) if dy == 1 else (0, 1):
            for quarter in range(2):
                at = pl.ds(1024 * half + 512 * quarter, 512)
                term = nn(memory_in, wom[:, at]) * scale + nn(pool_in, wop[:, at])
                part[dy, half, :, pl.ds(512 * quarter, 512)] = term.astype(BF16)
            if dy and half == dy % 3:
                rs[1 + dy - dy // 2].start()

    phase("drain")
    all_b = brecv.at[pl.ds(0, NSP - 1)]
    all_u = urecv.at[pl.ds(0, NSP - 1)]
    pltpu.make_async_copy(all_b, all_b, bsem.at[0]).wait()
    pltpu.make_async_copy(all_u, all_u, usem.at[0]).wait()
    pltpu.make_async_copy(all_u, all_u, ssem.at[0]).wait()
    for copy in w_copies + z_copies + [rs[6], rs[7]]:
        copy.wait_send()

    @pl.when(sp < NSP - 1)
    def _():
        halo.wait_send()

    pltpu.make_async_copy(psib, psib, psem.at[0]).wait()
    pltpu.make_async_copy(sqr, sqr, qsem.at[0]).wait()
    rs[6].wait_recv()
    rs[7].wait_recv()

    phase("rw0")
    rs[0].wait_recv()
    phase("fwd0")
    fwd[0] = (part[1, 0].astype(F32) + rp1[...].astype(F32) + out_scale(1) * r1[...].astype(F32)).astype(BF16)
    rs[4].start()
    phase("rw1")
    rs[1].wait_recv()
    phase("fwd1")
    fwd[1] = (part[3, 1].astype(F32) + rp2[...].astype(F32) + out_scale(3) * r2[...].astype(F32)).astype(BF16)
    rs[5].start()
    phase("rw2")
    for n in range(2, 4):
        rs[n].wait_recv()
    for n in range(4):
        rs[n].wait_send()
    phase("rw4")
    for n in range(4, 6):
        rs[n].wait_recv()
    phase("final")
    low = part[0, 0].astype(F32) + r4[...].astype(F32) + r5[...].astype(F32)
    high = part[0, 1].astype(F32) + r3[...].astype(F32) + r6[...].astype(F32)
    mean = (jnp.sum(low * low, axis=1, keepdims=True) + jnp.sum(high * high, axis=1, keepdims=True)) / D
    scale = lax.rsqrt(mean + EPS)
    out[:, 0:1024] = (low * scale * post[:, 0:1024]).astype(BF16)
    out[:, 1024:2048] = (high * scale * post[:, 1024:2048]).astype(BF16)
    for n in range(4, 6):
        rs[n].wait_send()
    phase(None)


def body(
    tokens, pre_gain, w_query, w_key, w_value, memory_output_gate_weight, w_input_gate, w_forget_gate, input_bias,
    forget_bias, forget_extra, initial_memory, initial_normal, memory_gain, w_pool_input, w_pool_gate, pool_mix,
    pool_gain, w_out_memory, w_out_pool, post_gain,
):
    args = (
        tokens, pre_gain.reshape(1, D), w_query, w_key, w_value, memory_output_gate_weight, w_input_gate.T,
        w_forget_gate.T, input_bias.reshape(1, 8), forget_bias.reshape(1, 8), forget_extra.reshape(8, 128),
        initial_memory.reshape(8, H), initial_normal, memory_gain.reshape(1, D), w_pool_input, w_pool_gate, pool_mix,
        pool_gain.reshape(1, NTP * G), w_out_memory, w_out_pool, post_gain.reshape(1, D),
    )
    vmem = pltpu.VMEM
    dma = pltpu.SemaphoreType.DMA
    scratch = [
        vmem((T, D), BF16), vmem((T, D), BF16), vmem((D, H), BF16), vmem((D, H), BF16), vmem((D, H), BF16),
        vmem((D, H), BF16), vmem((D, 2 * G), BF16), vmem((D, G), BF16), vmem((16, D), BF16), vmem((1, D), F32), vmem((1, 8), F32),
        vmem((1, 8), F32), vmem((8, 128), F32), vmem((8, H), F32), vmem((1, 8), F32), vmem((1, H), F32),
        vmem((G, G), BF16), vmem((1, G), F32), vmem((2 * H, D), BF16), vmem((2 * G, D), BF16), vmem((1, D), F32),
        vmem((T, 128), F32), vmem((T, H), BF16), vmem((T, H), BF16), vmem((T, H), BF16), vmem((T, H), F32),
        vmem((HALO + T, G), BF16), vmem((T, G), F32), vmem((T, H), F32), vmem((T, 128), F32), vmem((128, 128), F32),
        vmem((H, H), F32), vmem((NSP, 16, 128), BF16), vmem((NSP, 16, 128), BF16), vmem((4, 128), F32),
        vmem((NSP, 4, 128), F32), vmem((NSP, 16, 128), BF16), vmem((NSP, 16, 128), BF16), vmem((H, H), F32),
        vmem((8, 128), F32), vmem((NTP - 1, 8, 128), F32), vmem((NTP, 128, H), BF16), vmem((NY, 128, H), BF16),
        vmem((NTP, 128, G), BF16), vmem((NY, 128, G), BF16),
        vmem((2, 128, 1024), BF16), vmem((NY, 2, 128, 1024), BF16), vmem((2, 128, 1024), BF16), vmem((128, 1024), BF16), vmem((128, 1024), BF16),
        vmem((128, 1024), BF16), vmem((128, 1024), BF16), vmem((128, 1024), BF16), vmem((128, 1024), BF16),
        vmem((128, 1024), BF16), vmem((128, 1024), BF16),
        dma((20,)), dma((4,)), dma((2,)), dma((2,)), dma((3,)), dma((3,)), dma((2,)), dma((2,)), dma((2,)),
        dma((2 * NY,)), dma((2,)), dma((8,)), dma((8,)),
    ]
    anywhere = pl.BlockSpec(memory_space=pltpu.HBM)
    return pl.pallas_call(
        kernel,
        out_shape=jax.ShapeDtypeStruct((128, D), BF16),
        in_specs=[anywhere] * len(args),
        out_specs=pl.BlockSpec(memory_space=pltpu.VMEM),
        scratch_shapes=scratch,
        compiler_params=pltpu.CompilerParams(
            collective_id=0, has_side_effects=True, vmem_limit_bytes=48 * 1024 * 1024
        ),
    )(*[pltpu.with_memory_space_constraint(a, pltpu.HBM) for a in args])


def solution(mesh):
    in_specs = (
        P("sp", None), P(), P(None, "tp"), P(None, "tp"), P(None, "tp"), P(None, "tp"), P(), P(), P(), P(),
        P("sp", "tp"), P("tp", "sp", None), P("tp", "sp"), P(), P(None, "tp"), P(None, "tp"), P(), P(),
        P("tp", None), P("tp", None), P(),
    )
    return jax.shard_map(
        body, mesh=mesh, in_specs=in_specs, out_specs=P(("sp", "tp"), None), check_vma=False
    )
```

```python
import jax
import jax.numpy as jnp
from jax import lax
from jax.experimental import pallas as pl
from jax.experimental.pallas import tpu as pltpu
from jax.sharding import PartitionSpec as P

EPS = 1e-6
NEG = -1e30
F32 = jnp.float32
BF16 = jnp.bfloat16
MESH = pl.DeviceIdType.MESH

T = 1024
D = 2048
H = 256
G = 128
NSP = 32
NZ, NX = 8, 4
NTP = 8
NY = 4
HALF = NSP // 2
STAGES = ((0, 8), (8, 8), (16, 16))
CHUNKS = ((0, 256), (256, 256), (512, 256), (768, 256))
HALO = 256


def nn(a, b):
    return jnp.dot(a, b, preferred_element_type=F32)


def nt(a, b):
    return lax.dot_general(a, b, (((1,), (1,)), ((), ())), preferred_element_type=F32)


def tn(a, b):
    return lax.dot_general(a, b, (((0,), (0,)), ((), ())), preferred_element_type=F32)


def silu(x):
    return x / (1.0 + jnp.exp(-x))


class Phases:
    scope = None

    def __call__(self, name):
        if self.scope is not None:
            self.scope.__exit__(None, None, None)
        self.scope = jax.named_scope(name) if name else None
        if name:
            self.scope.__enter__()


def scan_packed(x, combine, fill):
    lane = lax.broadcasted_iota(jnp.int32, (8, 128), 1)
    sub = lax.broadcasted_iota(jnp.int32, (8, 128), 0)
    for step in (1, 2, 4, 8, 16, 32, 64):
        x = combine(x, jnp.where(lane >= step, pltpu.roll(x, step, 1), fill))
    rows = jnp.broadcast_to(x[:, 127:128], (8, 128))
    before = jnp.where(sub >= 1, pltpu.roll(rows, 1, 0), fill)
    for step in (1, 2, 4):
        before = combine(before, jnp.where(sub >= step, pltpu.roll(before, step, 0), fill))
    return combine(x, before)


def columns_of(packed):
    rows = jnp.concatenate(packed + [jnp.zeros((128 - 8 * len(packed), 128), F32)], axis=0)
    return rows.T


def kernel(
    tokens, pre_gain, w_query, w_key, w_value, w_gate, w_in, w_forget, in_bias, forget_bias, extra, init_memory,
    init_normal, memory_gain, w_pool_in, w_pool_gate, pool_mix, pool_gain, w_out_memory, w_out_pool, post_gain,
    out,
    tok, nrm, wq, wk, wv, wg, wp, wpg, gw, pre, bias_i, bias_f, fex, im, inn, mg, pm, pg, wom, wop, post,
    gz, q, k, v, gate, pool_ext, pgate, num, den, cols,
    ustate, usend, urecv, bsend, brecv, ssend, srecv, smat,
    sqs, sqr, zbuf, zsib, pbuf, psib, ppart, part, fwd, r1, r2, r3, r4, r5, r6, rp1, rp2,
    lsem, tsem, wsend, wrecv, usem, bsem, hsem, ssem, qsem, zsem, psem, rsend, rrecv,
):
    sp = lax.axis_index("sp")
    tp = lax.axis_index("tp")
    z, x = sp // NX, sp % NX
    y, c = tp // 2, tp % 2
    sib = {"sp": sp, "tp": 2 * y + (1 - c)}
    up = {"sp": sp, "tp": 2 * lax.rem(y + 1, NY) + c}
    down = {"sp": sp, "tp": 2 * lax.rem(y + NY - 1, NY) + c}

    def sp_peer(n):
        dz, dx = (4, 5, 3, 6, 2, 7, 1, 0)[n // NX], (2, 1, 3, 0)[n % NX]
        return lax.rem(z + dz, NZ) * NX + lax.rem(x + dx, NX)

    phase = Phases()
    phase("loads")
    tok_copies = [
        pltpu.make_async_copy(tokens.at[pl.ds(at, size)], tok.at[pl.ds(at, size)], tsem.at[i])
        for i, (at, size) in enumerate(CHUNKS)
    ]
    loads = [
        (pre_gain, pre), (w_in, gw.at[pl.ds(0, 8)]), (w_forget, gw.at[pl.ds(8, 8)]), (w_key, wk),
        (w_pool_in, wp.at[:, pl.ds(0, G)]), (w_value, wv),
        (in_bias, bias_i), (forget_bias, bias_f), (extra, fex), (init_memory, im), (init_normal, inn),
        (w_query, wq), (w_gate, wg), (w_pool_gate, wpg),
        (memory_gain.at[:, pl.ds(pl.multiple_of(tp * H, H), H)], mg), (pool_mix.at[tp], pm),
        (pool_gain.at[:, pl.ds(pl.multiple_of(tp * G, G), G)], pg),
        (w_out_memory, wom.at[pl.ds(0, H)]), (w_out_pool, wop.at[pl.ds(0, G)]), (post_gain, post),
    ]
    copies = [pltpu.make_async_copy(src, dst, lsem.at[i]) for i, (src, dst) in enumerate(loads)]
    tok_copies[0].start()
    for copy in (*copies[0:3], tok_copies[1], copies[3], copies[4], *tok_copies[2:]):
        copy.start()

    pool_ext[pl.ds(0, HALO), :] = jnp.zeros((HALO, G), BF16)
    phase("greet")
    barrier = pltpu.get_barrier_semaphore()

    for n in range(NSP - 1):
        pl.semaphore_signal(barrier, inc=1, device_id={"sp": sp_peer(n), "tp": tp}, device_id_type=MESH)
    for n in range(1, NTP):
        pl.semaphore_signal(barrier, inc=1, device_id={"sp": sp, "tp": lax.rem(tp + n, NTP)}, device_id_type=MESH)

    def norm_rows(i):
        tok_copies[i].wait()
        rows = pl.ds(*CHUNKS[i])
        total = jnp.zeros((CHUNKS[i][1], 128), F32)
        for col in range(D // 128):
            piece = tok[rows, pl.ds(128 * col, 128)].astype(F32)
            total = total + piece * piece
        scale = lax.rsqrt(jnp.sum(total, axis=1, keepdims=True) / D + EPS)
        for col in range(D // 128):
            at = pl.ds(128 * col, 128)
            piece = tok[rows, at].astype(F32)
            nrm[rows, at] = (piece * scale * pre[:, at]).astype(BF16)

    phase("norm0")
    copies[0].wait()
    norm_rows(0)
    for copy in copies[5:]:
        copy.start()
    for i in (4, 3):
        copies[i].wait()
    phase("gw")
    for i in (1, 2):
        copies[i].wait()
    for col in range(D // 128):
        at = pl.ds(128 * col, 128)
        logits = jnp.concatenate([gw[:, at].astype(F32), jnp.zeros((112, 128), F32)], axis=0)
        wp[at, G : 2 * G] = logits.T.astype(BF16)
    for i, (at, size) in enumerate(CHUNKS):
        phase("kv%d" % i)
        if i < 3:
            norm_rows(i + 1)
        rows = pl.ds(at, size)
        normed = nrm[rows, :]
        both = nn(normed, wp[...])
        pool_ext[pl.ds(HALO + at, size), :] = both[:, 0:G].astype(BF16)
        gz[rows, :] = both[:, G : 2 * G]
        k[rows, :] = nn(normed, wk[...]).astype(BF16)
    phase("gates")
    for i in range(5, 11):
        copies[i].wait()
    for i in range(2):
        rows = pl.ds(512 * i, 512)
        v[rows, :] = nn(nrm[rows, :], wv[...]).astype(BF16)

    head8 = lax.broadcasted_iota(jnp.int32, (8, 128), 0) == tp
    lin, lfor = [], []
    for r in range(8):
        block = gz[pl.ds(128 * r, 128), :].T
        lin.append(jnp.sum(jnp.where(head8, block[0:8], 0.0), axis=0, keepdims=True))
        lfor.append(jnp.sum(jnp.where(head8, block[8:16], 0.0), axis=0, keepdims=True))
    own8 = lax.broadcasted_iota(jnp.int32, (1, 8), 1) == tp
    shift_i = jnp.sum(jnp.where(own8, bias_i[...], 0.0), axis=1, keepdims=True)
    shift_f = jnp.sum(jnp.where(own8, bias_f[...], 0.0), axis=1, keepdims=True)
    log_input = jnp.concatenate(lin, axis=0) + shift_i
    pre_keep = jnp.concatenate(lfor, axis=0) + shift_f
    log_keep = jnp.minimum(pre_keep, 0.0) - jnp.log1p(jnp.exp(-jnp.abs(pre_keep))) + fex[...]
    keep_run = scan_packed(log_keep, jnp.add, 0.0)
    offer = log_input - keep_run
    keep_all = keep_run[7:8, 127:128]
    best_all = jnp.max(jnp.max(offer, axis=0, keepdims=True), axis=1, keepdims=True)
    write = jnp.exp(offer - best_all)
    colA = columns_of([write])

    def column(source, index, i):
        at = 8 * index + 2 * i
        return jnp.concatenate([source[:, at : at + 1], source[:, at + 1 : at + 2]], axis=0)

    phase("barrier")
    pl.semaphore_wait(barrier, NSP - 1 + NTP - 1)

    def halo_copy(size):
        return pltpu.make_async_remote_copy(
            src_ref=pool_ext.at[pl.ds(HALO + T - size, size)], dst_ref=pool_ext.at[pl.ds(HALO - size, size)],
            send_sem=hsem.at[0], recv_sem=hsem.at[1], device_id={"sp": lax.rem(sp + 1, NSP), "tp": tp},
            device_id_type=MESH,
        )

    def with_halo(there, act):
        @pl.when(there & (tp < 6))
        def _():
            act(halo_copy(64))

        @pl.when(there & (tp >= 6))
        def _():
            act(halo_copy(HALO))

    with_halo(sp < NSP - 1, lambda copy: copy.start())

    phase("state")
    state = jnp.zeros((H, H), F32)
    normal = jnp.zeros((1, H), F32)
    for i in range(4):
        rows = pl.ds(256 * i, 256)
        weighted = column(colA, 0, i) * k[rows, :].astype(F32)
        normal = normal + jnp.sum(weighted, axis=0, keepdims=True)
        state = state + tn(weighted.astype(BF16), v[rows, :])
    ustate[...] = state
    lane128 = lax.broadcasted_iota(jnp.int32, (1, 128), 1)
    bsend[0:1, :] = normal[:, 0:128]
    bsend[1:2, :] = normal[:, 128:256]
    bsend[2:3, :] = jnp.where(lane128 < 64, keep_all + best_all, keep_all)
    placed = jnp.concatenate([inn[...], jnp.zeros((1, 120), F32)], axis=1)
    bsend[3:4, :] = pltpu.roll(placed, 8 * lax.rem(sp, 16), 1)

    phase("pack")
    def pack_slab(j, carry):
        slab = ustate[pl.ds(pl.multiple_of(8 * j, 8), 8), :]
        usend[j] = jnp.concatenate([slab[:, 0:128], slab[:, 128:256]], axis=0).astype(BF16)
        return carry

    lax.fori_loop(0, NSP, pack_slab, 0)
    urecv[sp] = usend[sp]
    brecv[sp] = bsend[...]

    my_stage = jnp.where(sp < STAGES[1][0], 0, jnp.where(sp < STAGES[2][0], 1, 2))

    def b_copy(dst):
        return pltpu.make_async_remote_copy(
            src_ref=bsend, dst_ref=brecv.at[sp], send_sem=bsem.at[0], recv_sem=bsem.at[1 + my_stage],
            device_id={"sp": dst, "tp": tp}, device_id_type=MESH,
        )

    def u_copy(dst):
        return pltpu.make_async_remote_copy(
            src_ref=usend.at[dst], dst_ref=urecv.at[sp], send_sem=usem.at[0], recv_sem=usem.at[1 + my_stage],
            device_id={"sp": dst, "tp": tp}, device_id_type=MESH,
        )

    def s_copy(dst):
        return pltpu.make_async_remote_copy(
            src_ref=ssend.at[dst], dst_ref=srecv.at[sp], send_sem=ssem.at[0], recv_sem=ssem.at[1],
            device_id={"sp": dst, "tp": tp}, device_id_type=MESH,
        )

    def send_first():
        for n in range(NSP - 1):
            dst = sp_peer(n)
            b_copy(dst).start()
            u_copy(dst).start()

    def send_second(stage):
        first, size = STAGES[stage]
        for n in range(size):
            dst = first + lax.rem(sp + size // 2 + n, size)

            @pl.when(dst != sp)
            def _():
                s_copy(dst).start()

    def wait_first(stage):
        def wait(count):
            pltpu.make_async_copy(brecv.at[pl.ds(0, count)], brecv.at[pl.ds(0, count)], bsem.at[1 + stage]).wait()
            pltpu.make_async_copy(urecv.at[pl.ds(0, count)], urecv.at[pl.ds(0, count)], usem.at[1 + stage]).wait()

        @pl.when(my_stage == stage)
        def _():
            wait(STAGES[stage][1] - 1)

        @pl.when(my_stage != stage)
        def _():
            wait(STAGES[stage][1])

    phase("send1")
    send_first()
    w_copies = [
        pltpu.make_async_remote_copy(
            src_ref=src, dst_ref=dst, send_sem=wsend.at[i], recv_sem=wrecv.at[i], device_id=sib, device_id_type=MESH
        )
        for i, (src, dst) in enumerate([(w_out_memory, wom.at[pl.ds(H, H)]), (w_out_pool, wop.at[pl.ds(G, G)])])
    ]
    for copy in w_copies:
        copy.start()

    phase("pgate")
    for i in range(11, 17):
        copies[i].wait()
    for i in range(2):
        rows = pl.ds(512 * i, 512)
        pgate[rows, :] = silu(nn(nrm[rows, :], wpg[...])) * pg[...]

    def p_copy(n):
        return pltpu.make_async_remote_copy(
            src_ref=pbuf.at[2 * n + 1 - c], dst_ref=psib.at[n], send_sem=psem.at[0], recv_sem=psem.at[1],
            device_id=sib, device_id_type=MESH,
        )

    order = (2, 1, 3, 0)

    def rs_copy(n, src, dst, to):
        return pltpu.make_async_remote_copy(
            src_ref=src, dst_ref=dst, send_sem=rsend.at[n], recv_sem=rrecv.at[n], device_id=to, device_id_type=MESH
        )

    rs = [
        rs_copy(0, part.at[2, 0], r1, up), rs_copy(1, part.at[2, 1], r2, down),
        rs_copy(2, part.at[1, 1], r3, up), rs_copy(3, part.at[3, 0], r4, down),
        rs_copy(4, fwd.at[0], r5, up), rs_copy(5, fwd.at[1], r6, down),
        rs_copy(6, ppart.at[0], rp1, up), rs_copy(7, ppart.at[1], rp2, down),
    ]

    def memory_inputs(dy):
        to = lax.rem(y + dy, NY)
        return jnp.concatenate([zbuf[2 * to + c], zsib[to]], axis=1)

    def pool_inputs(dy):
        to = lax.rem(y + dy, NY)
        return jnp.concatenate([pbuf[2 * to + c], psib[to]], axis=1)

    phase("q")
    for i in range(2):
        rows = pl.ds(512 * i, 512)
        q[rows, :] = nn(nrm[rows, :], wq[...]).astype(BF16)

    phase("gate")
    for i in range(2):
        rows = pl.ds(512 * i, 512)
        gate[rows, :] = silu(nn(nrm[rows, :], wg[...])) * mg[...]

    memory = jnp.concatenate([im[:, 0:128], im[:, 128:256]], axis=0)
    stab = jnp.zeros((1, 1), F32)
    my_stab = jnp.zeros((1, 1), F32)
    carried_n = jnp.zeros((2, 128), F32)
    my_n = carried_n
    fade_all = jnp.ones((1, 1), F32)
    my_fade = fade_all
    best = scan_packed(offer, jnp.maximum, NEG)
    head_scale = H ** (-0.5)

    def beside():
        phase("pool")
        with_halo(sp > 0, lambda copy: copy.wait_recv())
        window = lax.shift_left(jnp.int32(2), tp)
        for i in range(4):
            rows = pl.ds(256 * i, 256)
            near = pool_ext[pl.ds(256 * i, 512), :]
            target = lax.broadcasted_iota(jnp.int32, (256, 512), 0) + HALO
            back = target - lax.broadcasted_iota(jnp.int32, (256, 512), 1)
            band = jnp.where((back >= 0) & (back < window), 1.0, 0.0).astype(BF16)
            sums = nn(band, near)
            place = sp * T + 256 * i + lax.broadcasted_iota(jnp.int32, (256, 1), 0) + 1
            count = jnp.minimum(place, window).astype(F32)
            pooled = (sums / count - near[HALO:, :].astype(F32)).astype(BF16)
            mixed = nn(pooled, pm[...]) * pgate[rows, :]
            pbuf[2 * i] = mixed[0:128].astype(BF16)
            pbuf[2 * i + 1] = mixed[128:256].astype(BF16)

        for n in range(NY):
            p_copy(n).start()

        phase("attn")
        colC = columns_of([best])
        for i in range(4):
            rows = pl.ds(256 * i, 256)
            length = 256 * (i + 1)
            scores = nt(q[rows, :], k[pl.ds(0, length), :])
            source = jnp.concatenate([offer[r : r + 1, :] for r in range(2 * (i + 1))], axis=1)
            exponent = source - column(colC, 0, i)
            ahead = lax.broadcasted_iota(jnp.int32, (256, length), 1) > lax.broadcasted_iota(
                jnp.int32, (256, length), 0
            ) + 256 * i
            weights = jnp.exp(jnp.where(ahead, NEG, exponent)) * scores * head_scale
            den[rows, :] = jnp.broadcast_to(jnp.sum(weights, axis=1, keepdims=True), (256, 128))
            num[rows, :] = nn(weights.astype(BF16), v[pl.ds(0, length), :])


    for stage, (first, size) in enumerate(STAGES):
        phase("wait1_%d" % stage)
        wait_first(stage)
        phase("scan%d" % stage)
        for j in range(first, first + size):
            mine = sp == j
            my_stab = jnp.where(mine, stab, my_stab)
            my_n = jnp.where(mine, carried_n, my_n)
            my_fade = jnp.where(mine, fade_all, my_fade)
            ssend[j] = memory.astype(BF16)
            piece_stab = brecv[j, 2:3, 0:1]
            piece_keep = brecv[j, 2:3, 64:65]
            new_stab = jnp.maximum(stab + piece_keep, piece_stab)
            fade = jnp.exp(stab + piece_keep - new_stab)
            weight = jnp.exp(piece_stab - new_stab)
            memory = fade * memory + weight * urecv[j].astype(F32)
            carried_n = fade * carried_n + weight * brecv[j, 0:2, :]
            fade_all = fade_all * fade
            stab = new_stab

        phase("send2_%d" % stage)

        @pl.when(my_stage == stage)
        def _():
            srecv[sp] = ssend[sp]

        send_second(stage)
        if stage == 1:
            pl.when(sp < HALF)(beside)
    pl.when(sp >= HALF)(beside)

    phase("pout")
    for i in range(17, 20):
        copies[i].wait()
    for copy in w_copies:
        copy.wait_recv()
    pltpu.make_async_copy(psib, psib, psem.at[1]).wait()
    pool_in = pool_inputs(2)
    for quarter in range(4):
        at = pl.ds(512 * (quarter % 2), 512)
        ppart[quarter // 2, :, at] = nn(pool_in, wop[:, pl.ds(512 * quarter, 512)]).astype(BF16)
    rs[6].start()
    rs[7].start()

    start_low = jnp.zeros((1, 128), F32)
    start_high = jnp.zeros((1, 128), F32)
    for j in range(HALF):
        start_low = start_low + brecv[j, 3:4, :]
        start_high = start_high + brecv[HALF + j, 3:4, :]
    my_n = my_n + my_fade * jnp.concatenate([start_low, start_high], axis=0)

    phase("denom")
    joint = jnp.maximum(best, my_stab)
    local_weight = jnp.exp(best - joint)
    carry_weight = jnp.exp(my_stab - joint) * head_scale
    least = jnp.exp(-(keep_run + joint))
    cols[...] = columns_of([local_weight, carry_weight, least])
    n_row = jnp.concatenate([my_n[0:1, :], my_n[1:2, :]], axis=1)
    colB = cols[...]
    for i in range(4):
        rows = pl.ds(256 * i, 256)
        carried = jnp.sum(q[rows, :].astype(F32) * n_row, axis=1, keepdims=True)
        full = den[rows, 0:1] * column(colB, 0, i) + column(colB, 1, i) * carried
        inverse = 1.0 / jnp.maximum(jnp.abs(full), column(colB, 2, i))
        num[rows, :] = num[rows, :] * (column(colB, 0, i) * inverse)
        den[rows, :] = jnp.broadcast_to(column(colB, 1, i) * inverse, (256, 128))

    phase("wait2")
    pltpu.make_async_copy(srecv.at[pl.ds(0, NSP - 1)], srecv.at[pl.ds(0, NSP - 1)], ssem.at[1]).wait()
    phase("finish")
    for j in range(NSP):
        slab = srecv[j].astype(F32)
        smat[8 * j : 8 * j + 8, 0:128] = slab[0:8]
        smat[8 * j : 8 * j + 8, 128:256] = slab[8:16]
    held = smat[...].astype(BF16)
    lane_sq = lax.broadcasted_iota(jnp.int32, (128, 128), 1)
    squares = jnp.zeros((128, 128), F32)

    def z_copy(n):
        to = lax.rem(y + order[n], NY)
        return pltpu.make_async_remote_copy(
            src_ref=zbuf.at[2 * to + 1 - c], dst_ref=zsib.at[to], send_sem=zsem.at[n], recv_sem=zsem.at[NY + n],
            device_id=sib, device_id_type=MESH,
        )

    z_copies = [z_copy(n) for n in range(NY)]
    for n in range(NY):
        for core in (1 - c, c):
            block = 2 * lax.rem(y + order[n], NY) + core
            rows = pl.ds(pl.multiple_of(128 * block, 128), 128)
            memory_rows = num[rows, :] + den[rows, 0:1] * nn(q[rows, :], held)
            sq = jnp.sum(memory_rows * memory_rows, axis=1, keepdims=True)
            squares = jnp.where(lane_sq == block, sq, squares)
            zbuf[block] = (memory_rows * gate[rows, :]).astype(BF16)
        z_copies[n].start()
    own_sq = squares.T[0:8]
    sqs[...] = own_sq

    def sq_copy(n):
        return pltpu.make_async_remote_copy(
            src_ref=sqs, dst_ref=sqr.at[n], send_sem=qsem.at[0], recv_sem=qsem.at[1],
            device_id={"sp": sp, "tp": lax.rem(tp + n + 1, NTP)}, device_id_type=MESH,
        )

    for n in range(NTP - 1):
        sq_copy(n).start()
    eye = lax.broadcasted_iota(jnp.int32, (128, 128), 0) == lax.broadcasted_iota(jnp.int32, (128, 128), 1)

    def out_scale(dy):
        to = lax.rem(y + dy, NY)
        row = cols[pl.ds(2 * to + c, 1), :]
        return jnp.sum(jnp.where(eye, jnp.broadcast_to(row, (128, 128)), 0.0), axis=1, keepdims=True)

    phase("zwait")
    z_copies[0].wait_recv()
    phase("ob2")
    memory_in = memory_inputs(2)
    for half in range(2):
        for quarter in range(2):
            at = pl.ds(512 * quarter, 512)
            part[2, half, :, at] = nn(memory_in, wom[:, pl.ds(1024 * half + 512 * quarter, 512)]).astype(BF16)
        rs[half].start()

    phase("sqwait")
    pltpu.make_async_copy(sqr, sqr, qsem.at[1]).wait()
    phase("scale")
    total = own_sq
    for n in range(NTP - 1):
        total = total + sqr[n]
    cols[0:8, :] = lax.rsqrt(total / (NTP * H) + EPS)
    for n, dy in ((1, 1), (2, 3), (3, 0)):
        phase("ob%d" % dy)
        z_copies[n].wait_recv()
        memory_in, pool_in = memory_inputs(dy), pool_inputs(dy)
        scale = out_scale(dy)
        for half in (1, 0) if dy == 1 else (0, 1):
            for quarter in range(2):
                at = pl.ds(1024 * half + 512 * quarter, 512)
                term = nn(memory_in, wom[:, at]) * scale + nn(pool_in, wop[:, at])
                part[dy, half, :, pl.ds(512 * quarter, 512)] = term.astype(BF16)
            if dy and half == dy % 3:
                rs[1 + dy - dy // 2].start()

    phase("drain")
    all_b = brecv.at[pl.ds(0, NSP - 1)]
    all_u = urecv.at[pl.ds(0, NSP - 1)]
    pltpu.make_async_copy(all_b, all_b, bsem.at[0]).wait()
    pltpu.make_async_copy(all_u, all_u, usem.at[0]).wait()
    pltpu.make_async_copy(all_u, all_u, ssem.at[0]).wait()
    for copy in w_copies + z_copies + [rs[6], rs[7]]:
        copy.wait_send()

    with_halo(sp < NSP - 1, lambda copy: copy.wait_send())
    pltpu.make_async_copy(psib, psib, psem.at[0]).wait()
    pltpu.make_async_copy(sqr, sqr, qsem.at[0]).wait()
    rs[6].wait_recv()
    rs[7].wait_recv()

    phase("rw0")
    rs[0].wait_recv()
    phase("fwd0")
    fwd[0] = (part[1, 0].astype(F32) + rp1[...].astype(F32) + out_scale(1) * r1[...].astype(F32)).astype(BF16)
    rs[4].start()
    phase("rw1")
    rs[1].wait_recv()
    phase("fwd1")
    fwd[1] = (part[3, 1].astype(F32) + rp2[...].astype(F32) + out_scale(3) * r2[...].astype(F32)).astype(BF16)
    rs[5].start()
    phase("rw2")
    for n in range(2, 4):
        rs[n].wait_recv()
    for n in range(4):
        rs[n].wait_send()
    phase("rw4")
    for n in range(4, 6):
        rs[n].wait_recv()
    phase("final")
    low = part[0, 0].astype(F32) + r4[...].astype(F32) + r5[...].astype(F32)
    high = part[0, 1].astype(F32) + r3[...].astype(F32) + r6[...].astype(F32)
    mean = (jnp.sum(low * low, axis=1, keepdims=True) + jnp.sum(high * high, axis=1, keepdims=True)) / D
    scale = lax.rsqrt(mean + EPS)
    out[:, 0:1024] = (low * scale * post[:, 0:1024]).astype(BF16)
    out[:, 1024:2048] = (high * scale * post[:, 1024:2048]).astype(BF16)
    for n in range(4, 6):
        rs[n].wait_send()
    phase(None)


def body(
    tokens, pre_gain, w_query, w_key, w_value, memory_output_gate_weight, w_input_gate, w_forget_gate, input_bias,
    forget_bias, forget_extra, initial_memory, initial_normal, memory_gain, w_pool_input, w_pool_gate, pool_mix,
    pool_gain, w_out_memory, w_out_pool, post_gain,
):
    args = (
        tokens, pre_gain.reshape(1, D), w_query, w_key, w_value, memory_output_gate_weight, w_input_gate.T,
        w_forget_gate.T, input_bias.reshape(1, 8), forget_bias.reshape(1, 8), forget_extra.reshape(8, 128),
        initial_memory.reshape(8, H), initial_normal, memory_gain.reshape(1, D), w_pool_input, w_pool_gate, pool_mix,
        pool_gain.reshape(1, NTP * G), w_out_memory, w_out_pool, post_gain.reshape(1, D),
    )
    vmem = pltpu.VMEM
    dma = pltpu.SemaphoreType.DMA
    scratch = [
        vmem((T, D), BF16), vmem((T, D), BF16), vmem((D, H), BF16), vmem((D, H), BF16), vmem((D, H), BF16),
        vmem((D, H), BF16), vmem((D, 2 * G), BF16), vmem((D, G), BF16), vmem((16, D), BF16), vmem((1, D), F32), vmem((1, 8), F32),
        vmem((1, 8), F32), vmem((8, 128), F32), vmem((8, H), F32), vmem((1, 8), F32), vmem((1, H), F32),
        vmem((G, G), BF16), vmem((1, G), F32), vmem((2 * H, D), BF16), vmem((2 * G, D), BF16), vmem((1, D), F32),
        vmem((T, 128), F32), vmem((T, H), BF16), vmem((T, H), BF16), vmem((T, H), BF16), vmem((T, H), F32),
        vmem((HALO + T, G), BF16), vmem((T, G), F32), vmem((T, H), F32), vmem((T, 128), F32), vmem((128, 128), F32),
        vmem((H, H), F32), vmem((NSP, 16, 128), BF16), vmem((NSP, 16, 128), BF16), vmem((4, 128), F32),
        vmem((NSP, 4, 128), F32), vmem((NSP, 16, 128), BF16), vmem((NSP, 16, 128), BF16), vmem((H, H), F32),
        vmem((8, 128), F32), vmem((NTP - 1, 8, 128), F32), vmem((NTP, 128, H), BF16), vmem((NY, 128, H), BF16),
        vmem((NTP, 128, G), BF16), vmem((NY, 128, G), BF16),
        vmem((2, 128, 1024), BF16), vmem((NY, 2, 128, 1024), BF16), vmem((2, 128, 1024), BF16), vmem((128, 1024), BF16), vmem((128, 1024), BF16),
        vmem((128, 1024), BF16), vmem((128, 1024), BF16), vmem((128, 1024), BF16), vmem((128, 1024), BF16),
        vmem((128, 1024), BF16), vmem((128, 1024), BF16),
        dma((20,)), dma((4,)), dma((2,)), dma((2,)), dma((4,)), dma((4,)), dma((2,)), dma((2,)), dma((2,)),
        dma((2 * NY,)), dma((2,)), dma((8,)), dma((8,)),
    ]
    anywhere = pl.BlockSpec(memory_space=pltpu.HBM)
    return pl.pallas_call(
        kernel,
        out_shape=jax.ShapeDtypeStruct((128, D), BF16),
        in_specs=[anywhere] * len(args),
        out_specs=pl.BlockSpec(memory_space=pltpu.VMEM),
        scratch_shapes=scratch,
        compiler_params=pltpu.CompilerParams(
            collective_id=0, has_side_effects=True, vmem_limit_bytes=48 * 1024 * 1024
        ),
    )(*[pltpu.with_memory_space_constraint(a, pltpu.HBM) for a in args])


def solution(mesh):
    in_specs = (
        P("sp", None), P(), P(None, "tp"), P(None, "tp"), P(None, "tp"), P(None, "tp"), P(), P(), P(), P(),
        P("sp", "tp"), P("tp", "sp", None), P("tp", "sp"), P(), P(None, "tp"), P(None, "tp"), P(), P(),
        P("tp", None), P("tp", None), P(),
    )
    return jax.shard_map(
        body, mesh=mesh, in_specs=in_specs, out_specs=P(("sp", "tp"), None), check_vma=False
    )
```

```python
import jax
import jax.numpy as jnp
from jax import lax
from jax.experimental import pallas as pl
from jax.experimental.pallas import tpu as pltpu
from jax.sharding import PartitionSpec as P

EPS = 1e-6
NEG = -1e30
F32 = jnp.float32
BF16 = jnp.bfloat16
MESH = pl.DeviceIdType.MESH

T = 1024
D = 2048
H = 256
G = 128
NSP = 32
NZ, NX = 8, 4
NTP = 8
NY = 4
HALF = NSP // 2
STAGES = ((0, 8), (8, 8), (16, 16))
CHUNKS = ((0, 256), (256, 256), (512, 256), (768, 256))
HALO = 256


def nn(a, b):
    return jnp.dot(a, b, preferred_element_type=F32)


def nt(a, b):
    return lax.dot_general(a, b, (((1,), (1,)), ((), ())), preferred_element_type=F32)


def tn(a, b):
    return lax.dot_general(a, b, (((0,), (0,)), ((), ())), preferred_element_type=F32)


def silu(x):
    return x / (1.0 + jnp.exp(-x))


class Phases:
    scope = None

    def __call__(self, name):
        if self.scope is not None:
            self.scope.__exit__(None, None, None)
        self.scope = jax.named_scope(name) if name else None
        if name:
            self.scope.__enter__()


def scan_packed(x, combine, fill):
    lane = lax.broadcasted_iota(jnp.int32, (8, 128), 1)
    sub = lax.broadcasted_iota(jnp.int32, (8, 128), 0)
    for step in (1, 2, 4, 8, 16, 32, 64):
        x = combine(x, jnp.where(lane >= step, pltpu.roll(x, step, 1), fill))
    rows = jnp.broadcast_to(x[:, 127:128], (8, 128))
    before = jnp.where(sub >= 1, pltpu.roll(rows, 1, 0), fill)
    for step in (1, 2, 4):
        before = combine(before, jnp.where(sub >= step, pltpu.roll(before, step, 0), fill))
    return combine(x, before)


def columns_of(packed):
    rows = jnp.concatenate(packed + [jnp.zeros((128 - 8 * len(packed), 128), F32)], axis=0)
    return rows.T


def kernel(
    tokens, pre_gain, w_query, w_key, w_value, w_gate, w_in, w_forget, in_bias, forget_bias, extra, init_memory,
    init_normal, memory_gain, w_pool_in, w_pool_gate, pool_mix, pool_gain, w_out_memory, w_out_pool, post_gain,
    out,
    tok, nrm, wq, wk, wv, wg, wp, wpg, gw, pre, bias_i, bias_f, fex, im, inn, mg, pm, pg, wom, wop, post,
    gz, q, k, v, gate, pool_ext, pgate, num, den, cols,
    ustate, usend, urecv, arow, arecv, nrow, nrecv, ssend, srecv, smat,
    sqs, sqr, zbuf, zsib, pbuf, psib, ppart, part, fwd, r1, r2, r3, r4, r5, r6, rp1, rp2,
    lsem, tsem, wsend, wrecv, usem, bsem, nsem, hsem, ssem, qsem, zsem, psem, rsend, rrecv,
):
    sp = lax.axis_index("sp")
    tp = lax.axis_index("tp")
    z, x = sp // NX, sp % NX
    y, c = tp // 2, tp % 2
    sib = {"sp": sp, "tp": 2 * y + (1 - c)}
    up = {"sp": sp, "tp": 2 * lax.rem(y + 1, NY) + c}
    down = {"sp": sp, "tp": 2 * lax.rem(y + NY - 1, NY) + c}

    def sp_peer(n):
        dz, dx = (4, 5, 3, 6, 2, 7, 1, 0)[n // NX], (2, 1, 3, 0)[n % NX]
        return lax.rem(z + dz, NZ) * NX + lax.rem(x + dx, NX)

    phase = Phases()
    phase("loads")
    tok_copies = [
        pltpu.make_async_copy(tokens.at[pl.ds(at, size)], tok.at[pl.ds(at, size)], tsem.at[i])
        for i, (at, size) in enumerate(((0, 128), (128, 128), *CHUNKS[1:]))
    ]
    loads = [
        (pre_gain, pre), (w_in, gw.at[pl.ds(0, 8)]), (w_forget, gw.at[pl.ds(8, 8)]), (w_key, wk),
        (w_pool_in, wp.at[:, pl.ds(0, G)]), (w_value, wv),
        (in_bias, bias_i), (forget_bias, bias_f), (extra, fex), (init_memory, im), (init_normal, inn),
        (w_query, wq), (w_gate, wg), (w_pool_gate, wpg),
        (memory_gain.at[:, pl.ds(pl.multiple_of(tp * H, H), H)], mg), (pool_mix.at[tp], pm),
        (pool_gain.at[:, pl.ds(pl.multiple_of(tp * G, G), G)], pg),
        (w_out_memory, wom.at[pl.ds(0, H)]), (w_out_pool, wop.at[pl.ds(0, G)]), (post_gain, post),
    ]
    copies = [pltpu.make_async_copy(src, dst, lsem.at[i]) for i, (src, dst) in enumerate(loads)]
    tok_copies[0].start()
    for copy in (copies[0], tok_copies[1], *copies[1:3], tok_copies[2], copies[3], copies[4], *tok_copies[3:]):
        copy.start()

    pool_ext[pl.ds(0, HALO), :] = jnp.zeros((HALO, G), BF16)
    phase("greet")
    barrier = pltpu.get_barrier_semaphore()

    for n in range(NSP - 1):
        pl.semaphore_signal(barrier, inc=1, device_id={"sp": sp_peer(n), "tp": tp}, device_id_type=MESH)
    for n in range(1, NTP):
        pl.semaphore_signal(barrier, inc=1, device_id={"sp": sp, "tp": lax.rem(tp + n, NTP)}, device_id_type=MESH)

    def norm_rows(i):
        for n in (0, 1) if i == 0 else (i + 1,):
            tok_copies[n].wait()
        rows = pl.ds(*CHUNKS[i])
        total = jnp.zeros((CHUNKS[i][1], 128), F32)
        for col in range(D // 128):
            piece = tok[rows, pl.ds(128 * col, 128)].astype(F32)
            total = total + piece * piece
        scale = lax.rsqrt(jnp.sum(total, axis=1, keepdims=True) / D + EPS)
        for col in range(D // 128):
            at = pl.ds(128 * col, 128)
            piece = tok[rows, at].astype(F32)
            nrm[rows, at] = (piece * scale * pre[:, at]).astype(BF16)

    phase("norm0")
    copies[0].wait()
    norm_rows(0)
    for copy in copies[5:]:
        copy.start()
    for i in (4, 3):
        copies[i].wait()
    phase("gw")
    for i in (1, 2):
        copies[i].wait()
    for col in range(D // 128):
        at = pl.ds(128 * col, 128)
        logits = jnp.concatenate([gw[:, at].astype(F32), jnp.zeros((112, 128), F32)], axis=0)
        wp[at, G : 2 * G] = logits.T.astype(BF16)
    for i, (at, size) in enumerate(CHUNKS):
        phase("kv%d" % i)
        if i < 3:
            norm_rows(i + 1)
        rows = pl.ds(at, size)
        normed = nrm[rows, :]
        both = nn(normed, wp[...])
        pool_ext[pl.ds(HALO + at, size), :] = both[:, 0:G].astype(BF16)
        gz[rows, :] = both[:, G : 2 * G]
        k[rows, :] = nn(normed, wk[...]).astype(BF16)
    phase("gates")
    for i in range(5, 11):
        copies[i].wait()
    for i in range(2):
        rows = pl.ds(512 * i, 512)
        v[rows, :] = nn(nrm[rows, :], wv[...]).astype(BF16)

    head8 = lax.broadcasted_iota(jnp.int32, (8, 128), 0) == tp
    lin, lfor = [], []
    for r in range(8):
        block = gz[pl.ds(128 * r, 128), :].T
        lin.append(jnp.sum(jnp.where(head8, block[0:8], 0.0), axis=0, keepdims=True))
        lfor.append(jnp.sum(jnp.where(head8, block[8:16], 0.0), axis=0, keepdims=True))
    own8 = lax.broadcasted_iota(jnp.int32, (1, 8), 1) == tp
    shift_i = jnp.sum(jnp.where(own8, bias_i[...], 0.0), axis=1, keepdims=True)
    shift_f = jnp.sum(jnp.where(own8, bias_f[...], 0.0), axis=1, keepdims=True)
    log_input = jnp.concatenate(lin, axis=0) + shift_i
    pre_keep = jnp.concatenate(lfor, axis=0) + shift_f
    log_keep = jnp.minimum(pre_keep, 0.0) - jnp.log1p(jnp.exp(-jnp.abs(pre_keep))) + fex[...]
    keep_run = scan_packed(log_keep, jnp.add, 0.0)
    offer = log_input - keep_run
    keep_all = keep_run[7:8, 127:128]
    best_all = jnp.max(jnp.max(offer, axis=0, keepdims=True), axis=1, keepdims=True)
    write = jnp.exp(offer - best_all)
    colA = columns_of([write])

    def column(source, index, i):
        at = 8 * index + 2 * i
        return jnp.concatenate([source[:, at : at + 1], source[:, at + 1 : at + 2]], axis=0)

    phase("barrier")
    pl.semaphore_wait(barrier, NSP - 1 + NTP - 1)

    def halo_copy(size):
        return pltpu.make_async_remote_copy(
            src_ref=pool_ext.at[pl.ds(HALO + T - size, size)], dst_ref=pool_ext.at[pl.ds(HALO - size, size)],
            send_sem=hsem.at[0], recv_sem=hsem.at[1], device_id={"sp": lax.rem(sp + 1, NSP), "tp": tp},
            device_id_type=MESH,
        )

    def with_halo(there, act):
        @pl.when(there & (tp < 6))
        def _():
            act(halo_copy(64))

        @pl.when(there & (tp >= 6))
        def _():
            act(halo_copy(HALO))

    with_halo(sp < NSP - 1, lambda copy: copy.start())

    phase("state")
    state = jnp.zeros((H, H), F32)
    normal = jnp.zeros((1, H), F32)
    for i in range(4):
        rows = pl.ds(256 * i, 256)
        weighted = column(colA, 0, i) * k[rows, :].astype(F32)
        normal = normal + jnp.sum(weighted, axis=0, keepdims=True)
        state = state + tn(weighted.astype(BF16), v[rows, :])
    ustate[...] = state
    lane128 = lax.broadcasted_iota(jnp.int32, (1, 128), 1)
    nrow[0:1, :] = normal[:, 0:128]
    nrow[1:2, :] = normal[:, 128:256]
    placed = pltpu.roll(jnp.concatenate([inn[...], jnp.zeros((1, 120), F32)], axis=1), 64 + 8 * lax.rem(sp, 8), 1)
    arow[...] = jnp.where(lane128 < 32, keep_all + best_all, jnp.where(lane128 < 64, keep_all, placed))

    phase("pack")
    def pack_slab(j, carry):
        slab = ustate[pl.ds(pl.multiple_of(8 * j, 8), 8), :]
        usend[j] = jnp.concatenate([slab[:, 0:128], slab[:, 128:256]], axis=0).astype(BF16)
        return carry

    lax.fori_loop(0, NSP, pack_slab, 0)
    urecv[sp] = usend[sp]
    arecv[sp] = arow[...]
    nrecv[sp] = nrow[...]

    my_stage = jnp.where(sp < STAGES[1][0], 0, jnp.where(sp < STAGES[2][0], 1, 2))

    def b_copy(dst):
        return pltpu.make_async_remote_copy(
            src_ref=arow, dst_ref=arecv.at[sp], send_sem=bsem.at[0], recv_sem=bsem.at[1 + my_stage],
            device_id={"sp": dst, "tp": tp}, device_id_type=MESH,
        )

    def n_copy(dst):
        return pltpu.make_async_remote_copy(
            src_ref=nrow, dst_ref=nrecv.at[sp], send_sem=nsem.at[0], recv_sem=nsem.at[1],
            device_id={"sp": dst, "tp": tp}, device_id_type=MESH,
        )

    def u_copy(dst):
        return pltpu.make_async_remote_copy(
            src_ref=usend.at[dst], dst_ref=urecv.at[sp], send_sem=usem.at[0], recv_sem=usem.at[1 + my_stage],
            device_id={"sp": dst, "tp": tp}, device_id_type=MESH,
        )

    def s_copy(dst):
        return pltpu.make_async_remote_copy(
            src_ref=ssend.at[dst], dst_ref=srecv.at[sp], send_sem=ssem.at[0], recv_sem=ssem.at[1],
            device_id={"sp": dst, "tp": tp}, device_id_type=MESH,
        )

    def send_first():
        for n in range(NSP - 1):
            dst = sp_peer(n)
            b_copy(dst).start()
            u_copy(dst).start()
        for n in range(NSP - 1):
            n_copy(sp_peer(n)).start()

    def send_second(stage):
        first, size = STAGES[stage]
        for n in range(size):
            dst = first + lax.rem(sp + size // 2 + n, size)

            @pl.when(dst != sp)
            def _():
                s_copy(dst).start()

    def wait_first(stage):
        def wait(count):
            pltpu.make_async_copy(arecv.at[pl.ds(0, count)], arecv.at[pl.ds(0, count)], bsem.at[1 + stage]).wait()
            pltpu.make_async_copy(urecv.at[pl.ds(0, count)], urecv.at[pl.ds(0, count)], usem.at[1 + stage]).wait()

        @pl.when(my_stage == stage)
        def _():
            wait(STAGES[stage][1] - 1)

        @pl.when(my_stage != stage)
        def _():
            wait(STAGES[stage][1])

    phase("send1")
    send_first()
    w_copies = [
        pltpu.make_async_remote_copy(
            src_ref=src, dst_ref=dst, send_sem=wsend.at[i], recv_sem=wrecv.at[i], device_id=sib, device_id_type=MESH
        )
        for i, (src, dst) in enumerate([(w_out_memory, wom.at[pl.ds(H, H)]), (w_out_pool, wop.at[pl.ds(G, G)])])
    ]
    for copy in w_copies:
        copy.start()

    phase("pgate")
    for i in range(11, 17):
        copies[i].wait()
    for i in range(2):
        rows = pl.ds(512 * i, 512)
        pgate[rows, :] = silu(nn(nrm[rows, :], wpg[...])) * pg[...]

    def p_copy(n):
        return pltpu.make_async_remote_copy(
            src_ref=pbuf.at[2 * n + 1 - c], dst_ref=psib.at[n], send_sem=psem.at[0], recv_sem=psem.at[1],
            device_id=sib, device_id_type=MESH,
        )

    order = (2, 1, 3, 0)

    def rs_copy(n, src, dst, to):
        return pltpu.make_async_remote_copy(
            src_ref=src, dst_ref=dst, send_sem=rsend.at[0], recv_sem=rrecv.at[n], device_id=to, device_id_type=MESH
        )

    rs = [
        rs_copy(0, part.at[2, 0], r1, up), rs_copy(1, part.at[2, 1], r2, down),
        rs_copy(2, part.at[1, 1], r3, up), rs_copy(3, part.at[3, 0], r4, down),
        rs_copy(4, fwd.at[0], r5, up), rs_copy(5, fwd.at[1], r6, down),
        rs_copy(6, ppart.at[0], rp1, up), rs_copy(7, ppart.at[1], rp2, down),
    ]

    def memory_inputs(dy):
        to = lax.rem(y + dy, NY)
        return jnp.concatenate([zbuf[2 * to + c], zsib[to]], axis=1)

    def pool_inputs(dy):
        to = lax.rem(y + dy, NY)
        return jnp.concatenate([pbuf[2 * to + c], psib[to]], axis=1)

    phase("q")
    for i in range(2):
        rows = pl.ds(512 * i, 512)
        q[rows, :] = nn(nrm[rows, :], wq[...]).astype(BF16)

    phase("gate")
    for i in range(2):
        rows = pl.ds(512 * i, 512)
        gate[rows, :] = silu(nn(nrm[rows, :], wg[...])) * mg[...]

    memory = jnp.concatenate([im[:, 0:128], im[:, 128:256]], axis=0)
    stab = jnp.zeros((1, 1), F32)
    my_stab = jnp.zeros((1, 1), F32)
    steps = []
    best = scan_packed(offer, jnp.maximum, NEG)
    head_scale = H ** (-0.5)

    def beside():
        phase("pool")
        with_halo(sp > 0, lambda copy: copy.wait_recv())
        window = lax.shift_left(jnp.int32(2), tp)
        for i in range(4):
            rows = pl.ds(256 * i, 256)
            near = pool_ext[pl.ds(256 * i, 512), :]
            target = lax.broadcasted_iota(jnp.int32, (256, 512), 0) + HALO
            back = target - lax.broadcasted_iota(jnp.int32, (256, 512), 1)
            band = jnp.where((back >= 0) & (back < window), 1.0, 0.0).astype(BF16)
            sums = nn(band, near)
            place = sp * T + 256 * i + lax.broadcasted_iota(jnp.int32, (256, 1), 0) + 1
            count = jnp.minimum(place, window).astype(F32)
            pooled = (sums / count - near[HALO:, :].astype(F32)).astype(BF16)
            mixed = nn(pooled, pm[...]) * pgate[rows, :]
            pbuf[2 * i] = mixed[0:128].astype(BF16)
            pbuf[2 * i + 1] = mixed[128:256].astype(BF16)

        for n in range(NY):
            p_copy(n).start()

        phase("attn")
        colC = columns_of([best])
        for i in range(4):
            rows = pl.ds(256 * i, 256)
            length = 256 * (i + 1)
            scores = nt(q[rows, :], k[pl.ds(0, length), :])
            source = jnp.concatenate([offer[r : r + 1, :] for r in range(2 * (i + 1))], axis=1)
            exponent = source - column(colC, 0, i)
            ahead = lax.broadcasted_iota(jnp.int32, (256, length), 1) > lax.broadcasted_iota(
                jnp.int32, (256, length), 0
            ) + 256 * i
            weights = jnp.exp(jnp.where(ahead, NEG, exponent)) * scores * head_scale
            den[rows, :] = jnp.broadcast_to(jnp.sum(weights, axis=1, keepdims=True), (256, 128))
            num[rows, :] = nn(weights.astype(BF16), v[pl.ds(0, length), :])

    for stage, (first, size) in enumerate(STAGES):
        phase("wait1_%d" % stage)
        wait_first(stage)
        phase("scan%d" % stage)
        for j in range(first, first + size):
            mine = sp == j
            my_stab = jnp.where(mine, stab, my_stab)
            ssend[j] = memory.astype(BF16)
            piece_stab = arecv[j, :, 0:1]
            piece_keep = arecv[j, :, 32:33]
            new_stab = jnp.maximum(stab + piece_keep, piece_stab)
            fade = jnp.exp(stab + piece_keep - new_stab)
            weight = jnp.exp(piece_stab - new_stab)
            memory = fade * memory + weight * urecv[j].astype(F32)
            steps.append((fade, weight))
            stab = new_stab

        phase("send2_%d" % stage)

        @pl.when(my_stage == stage)
        def _():
            srecv[sp] = ssend[sp]

        send_second(stage)
        if stage == 1:
            pl.when(sp < HALF)(beside)
    pl.when(sp >= HALF)(beside)

    phase("pout")
    for i in range(17, 20):
        copies[i].wait()
    for copy in w_copies:
        copy.wait_recv()
    pltpu.make_async_copy(psib, psib, psem.at[1]).wait()
    pool_in = pool_inputs(2)
    for quarter in range(4):
        at = pl.ds(512 * (quarter % 2), 512)
        ppart[quarter // 2, :, at] = nn(pool_in, wop[:, pl.ds(512 * quarter, 512)]).astype(BF16)
    rs[6].start()
    rs[7].start()

    phase("denom")
    pltpu.make_async_copy(nrecv.at[pl.ds(0, NSP - 1)], nrecv.at[pl.ds(0, NSP - 1)], nsem.at[1]).wait()
    quarters = []
    for first in range(0, NSP, 8):
        total = arecv[first]
        for j in range(first + 1, first + 8):
            total = total + arecv[j]
        quarters.append(total)
    my_n = jnp.concatenate(
        [jnp.where(lane128 < 64, pltpu.roll(quarters[n], 64, 1), quarters[n + 1]) for n in (0, 2)], axis=0
    )
    for j, (fade, weight) in enumerate(steps[: NSP - 1]):
        my_n = jnp.where(sp > j, fade * my_n + weight * nrecv[j], my_n)
    joint = jnp.maximum(best, my_stab)
    local_weight = jnp.exp(best - joint)
    carry_weight = jnp.exp(my_stab - joint) * head_scale
    least = jnp.exp(-(keep_run + joint))
    cols[...] = columns_of([local_weight, carry_weight, least])
    n_row = jnp.concatenate([my_n[0:1, :], my_n[1:2, :]], axis=1)
    n_top = n_row.astype(BF16)
    n_mid = (n_row - n_top.astype(F32)).astype(BF16)
    n_low = (n_row - n_top.astype(F32) - n_mid.astype(F32)).astype(BF16)
    n_rows = jnp.concatenate([n_top, n_mid, n_low, jnp.zeros((13, H), BF16)], axis=0)
    colB = cols[...]
    for i in range(4):
        rows = pl.ds(256 * i, 256)
        carried = jnp.sum(nt(q[rows, :], n_rows), axis=1, keepdims=True)
        full = den[rows, 0:1] * column(colB, 0, i) + column(colB, 1, i) * carried
        inverse = 1.0 / jnp.maximum(jnp.abs(full), column(colB, 2, i))
        num[rows, :] = num[rows, :] * (column(colB, 0, i) * inverse)
        den[rows, :] = jnp.broadcast_to(column(colB, 1, i) * inverse, (256, 128))

    phase("wait2")
    pltpu.make_async_copy(srecv.at[pl.ds(0, NSP - 1)], srecv.at[pl.ds(0, NSP - 1)], ssem.at[1]).wait()
    phase("finish")
    for j in range(NSP):
        slab = srecv[j].astype(F32)
        smat[8 * j : 8 * j + 8, 0:128] = slab[0:8]
        smat[8 * j : 8 * j + 8, 128:256] = slab[8:16]
    held = smat[...].astype(BF16)
    lane_sq = lax.broadcasted_iota(jnp.int32, (128, 128), 1)
    squares = jnp.zeros((128, 128), F32)

    def z_copy(n):
        to = lax.rem(y + order[n], NY)
        return pltpu.make_async_remote_copy(
            src_ref=zbuf.at[2 * to + 1 - c], dst_ref=zsib.at[to], send_sem=zsem.at[NY], recv_sem=zsem.at[n],
            device_id=sib, device_id_type=MESH,
        )

    z_copies = [z_copy(n) for n in range(NY)]
    for n in range(NY):
        for core in (1 - c, c):
            block = 2 * lax.rem(y + order[n], NY) + core
            rows = pl.ds(pl.multiple_of(128 * block, 128), 128)
            memory_rows = num[rows, :] + den[rows, 0:1] * nn(q[rows, :], held)
            sq = jnp.sum(memory_rows * memory_rows, axis=1, keepdims=True)
            squares = jnp.where(lane_sq == block, sq, squares)
            zbuf[block] = (memory_rows * gate[rows, :]).astype(BF16)
        z_copies[n].start()
    own_sq = squares.T[0:8]
    sqs[...] = own_sq

    def sq_copy(n):
        return pltpu.make_async_remote_copy(
            src_ref=sqs, dst_ref=sqr.at[n], send_sem=qsem.at[0], recv_sem=qsem.at[1],
            device_id={"sp": sp, "tp": lax.rem(tp + n + 1, NTP)}, device_id_type=MESH,
        )

    for n in range(NTP - 1):
        sq_copy(n).start()
    eye = lax.broadcasted_iota(jnp.int32, (128, 128), 0) == lax.broadcasted_iota(jnp.int32, (128, 128), 1)

    def out_scale(dy):
        to = lax.rem(y + dy, NY)
        row = cols[pl.ds(2 * to + c, 1), :]
        return jnp.sum(jnp.where(eye, jnp.broadcast_to(row, (128, 128)), 0.0), axis=1, keepdims=True)

    phase("zwait")
    z_copies[0].wait_recv()
    phase("ob2")
    memory_in = memory_inputs(2)
    for half in range(2):
        for quarter in range(2):
            at = pl.ds(512 * quarter, 512)
            part[2, half, :, at] = nn(memory_in, wom[:, pl.ds(1024 * half + 512 * quarter, 512)]).astype(BF16)
        rs[half].start()

    phase("sqwait")
    pltpu.make_async_copy(sqr, sqr, qsem.at[1]).wait()
    phase("scale")
    total = own_sq
    for n in range(NTP - 1):
        total = total + sqr[n]
    cols[0:8, :] = lax.rsqrt(total / (NTP * H) + EPS)
    for n, dy in ((1, 1), (2, 3), (3, 0)):
        phase("ob%d" % dy)
        z_copies[n].wait_recv()
        memory_in, pool_in = memory_inputs(dy), pool_inputs(dy)
        scale = out_scale(dy)
        for half in (1, 0) if dy == 1 else (0, 1):
            for quarter in range(2):
                at = pl.ds(1024 * half + 512 * quarter, 512)
                term = nn(memory_in, wom[:, at]) * scale + nn(pool_in, wop[:, at])
                part[dy, half, :, pl.ds(512 * quarter, 512)] = term.astype(BF16)
            if dy and half == dy % 3:
                rs[1 + dy - dy // 2].start()

    phase("drain")
    all_b = arecv.at[pl.ds(0, NSP - 1)]
    pltpu.make_async_copy(nrecv.at[pl.ds(0, NSP - 1)], nrecv.at[pl.ds(0, NSP - 1)], nsem.at[0]).wait()
    all_u = urecv.at[pl.ds(0, NSP - 1)]
    pltpu.make_async_copy(all_b, all_b, bsem.at[0]).wait()
    pltpu.make_async_copy(all_u, all_u, usem.at[0]).wait()
    pltpu.make_async_copy(all_u, all_u, ssem.at[0]).wait()
    for copy in w_copies:
        copy.wait_send()
    pltpu.make_async_copy(zsib, zsib, zsem.at[NY]).wait()

    with_halo(sp < NSP - 1, lambda copy: copy.wait_send())
    pltpu.make_async_copy(psib, psib, psem.at[0]).wait()
    pltpu.make_async_copy(sqr, sqr, qsem.at[0]).wait()
    rs[6].wait_recv()
    rs[7].wait_recv()

    phase("rw0")
    rs[0].wait_recv()
    phase("fwd0")
    fwd[0] = (part[1, 0].astype(F32) + rp1[...].astype(F32) + out_scale(1) * r1[...].astype(F32)).astype(BF16)
    rs[4].start()
    phase("rw1")
    rs[1].wait_recv()
    phase("fwd1")
    fwd[1] = (part[3, 1].astype(F32) + rp2[...].astype(F32) + out_scale(3) * r2[...].astype(F32)).astype(BF16)
    rs[5].start()
    phase("rw2")
    for n in range(2, 4):
        rs[n].wait_recv()
    low = part[0, 0].astype(F32) + r4[...].astype(F32)
    high = part[0, 1].astype(F32) + r3[...].astype(F32)
    phase("rw4")
    for n in range(4, 6):
        rs[n].wait_recv()
    phase("final")
    low = low + r5[...].astype(F32)
    high = high + r6[...].astype(F32)
    mean = (jnp.sum(low * low, axis=1, keepdims=True) + jnp.sum(high * high, axis=1, keepdims=True)) / D
    scale = lax.rsqrt(mean + EPS)
    out[:, 0:1024] = (low * scale * post[:, 0:1024]).astype(BF16)
    out[:, 1024:2048] = (high * scale * post[:, 1024:2048]).astype(BF16)
    pltpu.make_async_copy(part, part, rsend.at[0]).wait()
    phase(None)


def body(
    tokens, pre_gain, w_query, w_key, w_value, memory_output_gate_weight, w_input_gate, w_forget_gate, input_bias,
    forget_bias, forget_extra, initial_memory, initial_normal, memory_gain, w_pool_input, w_pool_gate, pool_mix,
    pool_gain, w_out_memory, w_out_pool, post_gain,
):
    args = (
        tokens, pre_gain.reshape(1, D), w_query, w_key, w_value, memory_output_gate_weight, w_input_gate.T,
        w_forget_gate.T, input_bias.reshape(1, 8), forget_bias.reshape(1, 8), forget_extra.reshape(8, 128),
        initial_memory.reshape(8, H), initial_normal, memory_gain.reshape(1, D), w_pool_input, w_pool_gate, pool_mix,
        pool_gain.reshape(1, NTP * G), w_out_memory, w_out_pool, post_gain.reshape(1, D),
    )
    vmem = pltpu.VMEM
    dma = pltpu.SemaphoreType.DMA
    scratch = [
        vmem((T, D), BF16), vmem((T, D), BF16), vmem((D, H), BF16), vmem((D, H), BF16), vmem((D, H), BF16),
        vmem((D, H), BF16), vmem((D, 2 * G), BF16), vmem((D, G), BF16), vmem((16, D), BF16), vmem((1, D), F32), vmem((1, 8), F32),
        vmem((1, 8), F32), vmem((8, 128), F32), vmem((8, H), F32), vmem((1, 8), F32), vmem((1, H), F32),
        vmem((G, G), BF16), vmem((1, G), F32), vmem((2 * H, D), BF16), vmem((2 * G, D), BF16), vmem((1, D), F32),
        vmem((T, 128), F32), vmem((T, H), BF16), vmem((T, H), BF16), vmem((T, H), BF16), vmem((T, H), F32),
        vmem((HALO + T, G), BF16), vmem((T, G), F32), vmem((T, H), F32), vmem((T, 128), F32), vmem((128, 128), F32),
        vmem((H, H), F32), vmem((NSP, 16, 128), BF16), vmem((NSP, 16, 128), BF16), vmem((1, 128), F32),
        vmem((NSP, 1, 128), F32), vmem((2, 128), F32), vmem((NSP, 2, 128), F32), vmem((NSP, 16, 128), BF16), vmem((NSP, 16, 128), BF16), vmem((H, H), F32),
        vmem((8, 128), F32), vmem((NTP - 1, 8, 128), F32), vmem((NTP, 128, H), BF16), vmem((NY, 128, H), BF16),
        vmem((NTP, 128, G), BF16), vmem((NY, 128, G), BF16),
        vmem((2, 128, 1024), BF16), vmem((NY, 2, 128, 1024), BF16), vmem((2, 128, 1024), BF16), vmem((128, 1024), BF16), vmem((128, 1024), BF16),
        vmem((128, 1024), BF16), vmem((128, 1024), BF16), vmem((128, 1024), BF16), vmem((128, 1024), BF16),
        vmem((128, 1024), BF16), vmem((128, 1024), BF16),
        dma((20,)), dma((5,)), dma((2,)), dma((2,)), dma((4,)), dma((4,)), dma((2,)), dma((2,)), dma((2,)), dma((2,)),
        dma((NY + 1,)), dma((2,)), dma((1,)), dma((8,)),
    ]
    anywhere = pl.BlockSpec(memory_space=pltpu.HBM)
    return pl.pallas_call(
        kernel,
        out_shape=jax.ShapeDtypeStruct((128, D), BF16),
        in_specs=[anywhere] * len(args),
        out_specs=pl.BlockSpec(memory_space=pltpu.VMEM),
        scratch_shapes=scratch,
        compiler_params=pltpu.CompilerParams(
            collective_id=0, has_side_effects=True, vmem_limit_bytes=48 * 1024 * 1024
        ),
    )(*[pltpu.with_memory_space_constraint(a, pltpu.HBM) for a in args])


def solution(mesh):
    in_specs = (
        P("sp", None), P(), P(None, "tp"), P(None, "tp"), P(None, "tp"), P(None, "tp"), P(), P(), P(), P(),
        P("sp", "tp"), P("tp", "sp", None), P("tp", "sp"), P(), P(None, "tp"), P(None, "tp"), P(), P(),
        P("tp", None), P("tp", None), P(),
    )
    return jax.shard_map(
        body, mesh=mesh, in_specs=in_specs, out_specs=P(("sp", "tp"), None), check_vma=False
    )
```

```python
import jax
import jax.numpy as jnp
from jax import lax
from jax.experimental import pallas as pl
from jax.experimental.pallas import tpu as pltpu
from jax.sharding import PartitionSpec as P

EPS = 1e-6
NEG = -1e30
F32 = jnp.float32
BF16 = jnp.bfloat16
MESH = pl.DeviceIdType.MESH

T = 1024
D = 2048
H = 256
G = 128
NSP = 32
NZ, NX = 8, 4
NTP = 8
NY = 4
HALF = NSP // 2
STAGES = ((0, 8), (8, 8), (16, 16))
CHUNKS = ((0, 256), (256, 256), (512, 256), (768, 256))
HALO = 256


def nn(a, b):
    return jnp.dot(a, b, preferred_element_type=F32)


def nt(a, b):
    return lax.dot_general(a, b, (((1,), (1,)), ((), ())), preferred_element_type=F32)


def tn(a, b):
    return lax.dot_general(a, b, (((0,), (0,)), ((), ())), preferred_element_type=F32)


def silu(x):
    return x / (1.0 + jnp.exp(-x))


class Phases:
    scope = None

    def __call__(self, name):
        if self.scope is not None:
            self.scope.__exit__(None, None, None)
        self.scope = jax.named_scope(name) if name else None
        if name:
            self.scope.__enter__()


def scan_packed(x, combine, fill):
    lane = lax.broadcasted_iota(jnp.int32, (8, 128), 1)
    sub = lax.broadcasted_iota(jnp.int32, (8, 128), 0)
    for step in (1, 2, 4, 8, 16, 32, 64):
        x = combine(x, jnp.where(lane >= step, pltpu.roll(x, step, 1), fill))
    rows = jnp.broadcast_to(x[:, 127:128], (8, 128))
    before = jnp.where(sub >= 1, pltpu.roll(rows, 1, 0), fill)
    for step in (1, 2, 4):
        before = combine(before, jnp.where(sub >= step, pltpu.roll(before, step, 0), fill))
    return combine(x, before)


def columns_of(packed):
    rows = jnp.concatenate(packed + [jnp.zeros((128 - 8 * len(packed), 128), F32)], axis=0)
    return rows.T


def kernel(
    tokens, pre_gain, w_query, w_key, w_value, w_gate, w_in, w_forget, in_bias, forget_bias, extra, init_memory,
    init_normal, memory_gain, w_pool_in, w_pool_gate, pool_mix, pool_gain, w_out_memory, w_out_pool, post_gain,
    out,
    tok, nrm, wq, wk, wv, wg, wp, wpg, gw, pre, bias_i, bias_f, fex, im, inn, mg, pm, pg, wom, wop, post,
    gz, q, k, v, gate, pool_ext, pgate, num, den, cols,
    ustate, usend, urecv, arow, arecv, nrow, nrecv, ssend, srecv, smat,
    sqs, sqr, zbuf, zsib, pbuf, psib, ppart, part, fwd, r1, r2, r3, r4, r5, r6, rp1, rp2,
    lsem, tsem, wsend, wrecv, usem, bsem, nsem, hsem, ssem, qsem, zsem, psem, rsend, rrecv,
):
    sp = lax.axis_index("sp")
    tp = lax.axis_index("tp")
    z, x = sp // NX, sp % NX
    y, c = tp // 2, tp % 2
    sib = {"sp": sp, "tp": 2 * y + (1 - c)}
    up = {"sp": sp, "tp": 2 * lax.rem(y + 1, NY) + c}
    down = {"sp": sp, "tp": 2 * lax.rem(y + NY - 1, NY) + c}

    def sp_peer(n):
        dz, dx = (4, 5, 3, 6, 2, 7, 1, 0)[n // NX], (2, 1, 3, 0)[n % NX]
        return lax.rem(z + dz, NZ) * NX + lax.rem(x + dx, NX)

    phase = Phases()
    phase("loads")
    tok_copies = [
        pltpu.make_async_copy(tokens.at[pl.ds(at, size)], tok.at[pl.ds(at, size)], tsem.at[i])
        for i, (at, size) in enumerate(((0, 128), (128, 128), *CHUNKS[1:]))
    ]
    loads = [
        (pre_gain, pre), (w_in, gw.at[pl.ds(0, 8)]), (w_forget, gw.at[pl.ds(8, 8)]), (w_key, wk),
        (w_pool_in, wp.at[:, pl.ds(0, G)]), (w_value, wv),
        (in_bias, bias_i), (forget_bias, bias_f), (extra, fex), (init_memory, im), (init_normal, inn),
        (w_query, wq), (w_gate, wg), (w_pool_gate, wpg),
        (memory_gain.at[:, pl.ds(pl.multiple_of(tp * H, H), H)], mg), (pool_mix.at[tp], pm),
        (pool_gain.at[:, pl.ds(pl.multiple_of(tp * G, G), G)], pg),
        (w_out_memory, wom.at[pl.ds(0, H)]), (w_out_pool, wop.at[pl.ds(0, G)]), (post_gain, post),
    ]
    copies = [pltpu.make_async_copy(src, dst, lsem.at[i]) for i, (src, dst) in enumerate(loads)]
    tok_copies[0].start()
    for copy in (copies[0], tok_copies[1], *copies[1:3], tok_copies[2], copies[3], copies[4], *tok_copies[3:]):
        copy.start()

    pool_ext[pl.ds(0, HALO), :] = jnp.zeros((HALO, G), BF16)
    phase("greet")
    barrier = pltpu.get_barrier_semaphore()

    for n in range(NSP - 1):
        pl.semaphore_signal(barrier, inc=1, device_id={"sp": sp_peer(n), "tp": tp}, device_id_type=MESH)
    for n in range(1, NTP):
        pl.semaphore_signal(barrier, inc=1, device_id={"sp": sp, "tp": lax.rem(tp + n, NTP)}, device_id_type=MESH)

    def norm_rows(i):
        for n in (0, 1) if i == 0 else (i + 1,):
            tok_copies[n].wait()
        rows = pl.ds(*CHUNKS[i])
        total = jnp.zeros((CHUNKS[i][1], 128), F32)
        for col in range(D // 128):
            piece = tok[rows, pl.ds(128 * col, 128)].astype(F32)
            total = total + piece * piece
        scale = lax.rsqrt(jnp.sum(total, axis=1, keepdims=True) / D + EPS)
        for col in range(D // 128):
            at = pl.ds(128 * col, 128)
            piece = tok[rows, at].astype(F32)
            nrm[rows, at] = (piece * scale * pre[:, at]).astype(BF16)

    phase("norm0")
    copies[0].wait()
    norm_rows(0)
    for copy in copies[5:]:
        copy.start()
    for i in (4, 3):
        copies[i].wait()
    phase("gw")
    for i in (1, 2):
        copies[i].wait()
    for col in range(D // 128):
        at = pl.ds(128 * col, 128)
        logits = jnp.concatenate([gw[:, at].astype(F32), jnp.zeros((112, 128), F32)], axis=0)
        wp[at, G : 2 * G] = logits.T.astype(BF16)
    for i, (at, size) in enumerate(CHUNKS):
        phase("kv%d" % i)
        if i < 3:
            norm_rows(i + 1)
        rows = pl.ds(at, size)
        normed = nrm[rows, :]
        both = nn(normed, wp[...])
        pool_ext[pl.ds(HALO + at, size), :] = both[:, 0:G].astype(BF16)
        gz[rows, :] = both[:, G : 2 * G]
        k[rows, :] = nn(normed, wk[...]).astype(BF16)
    phase("gates")
    for i in range(5, 11):
        copies[i].wait()
    for i in range(2):
        rows = pl.ds(512 * i, 512)
        v[rows, :] = nn(nrm[rows, :], wv[...]).astype(BF16)

    head8 = lax.broadcasted_iota(jnp.int32, (8, 128), 0) == tp
    lin, lfor = [], []
    for r in range(8):
        block = gz[pl.ds(128 * r, 128), :].T
        lin.append(jnp.sum(jnp.where(head8, block[0:8], 0.0), axis=0, keepdims=True))
        lfor.append(jnp.sum(jnp.where(head8, block[8:16], 0.0), axis=0, keepdims=True))
    own8 = lax.broadcasted_iota(jnp.int32, (1, 8), 1) == tp
    shift_i = jnp.sum(jnp.where(own8, bias_i[...], 0.0), axis=1, keepdims=True)
    shift_f = jnp.sum(jnp.where(own8, bias_f[...], 0.0), axis=1, keepdims=True)
    log_input = jnp.concatenate(lin, axis=0) + shift_i
    pre_keep = jnp.concatenate(lfor, axis=0) + shift_f
    log_keep = jnp.minimum(pre_keep, 0.0) - jnp.log1p(jnp.exp(-jnp.abs(pre_keep))) + fex[...]
    keep_run = scan_packed(log_keep, jnp.add, 0.0)
    offer = log_input - keep_run
    keep_all = keep_run[7:8, 127:128]
    best_all = jnp.max(jnp.max(offer, axis=0, keepdims=True), axis=1, keepdims=True)
    write = jnp.exp(offer - best_all)
    colA = columns_of([write])

    def column(source, index, i):
        at = 8 * index + 2 * i
        return jnp.concatenate([source[:, at : at + 1], source[:, at + 1 : at + 2]], axis=0)

    phase("barrier")
    pl.semaphore_wait(barrier, NSP - 1 + NTP - 1)

    def halo_copy(size):
        return pltpu.make_async_remote_copy(
            src_ref=pool_ext.at[pl.ds(HALO + T - size, size)], dst_ref=pool_ext.at[pl.ds(HALO - size, size)],
            send_sem=hsem.at[0], recv_sem=hsem.at[1], device_id={"sp": lax.rem(sp + 1, NSP), "tp": tp},
            device_id_type=MESH,
        )

    def with_halo(there, act):
        @pl.when(there & (tp < 6))
        def _():
            act(halo_copy(64))

        @pl.when(there & (tp >= 6))
        def _():
            act(halo_copy(HALO))

    with_halo(sp < NSP - 1, lambda copy: copy.start())

    phase("state")
    state = jnp.zeros((H, H), F32)
    normal = jnp.zeros((1, H), F32)
    for i in range(4):
        rows = pl.ds(256 * i, 256)
        weighted = column(colA, 0, i) * k[rows, :].astype(F32)
        normal = normal + jnp.sum(weighted, axis=0, keepdims=True)
        state = state + tn(weighted.astype(BF16), v[rows, :])
    ustate[...] = state
    lane128 = lax.broadcasted_iota(jnp.int32, (1, 128), 1)
    nrow[0:1, :] = normal[:, 0:128]
    nrow[1:2, :] = normal[:, 128:256]
    placed = pltpu.roll(jnp.concatenate([inn[...], jnp.zeros((1, 120), F32)], axis=1), 64 + 8 * lax.rem(sp, 8), 1)
    arow[...] = jnp.where(lane128 < 32, keep_all + best_all, jnp.where(lane128 < 64, keep_all, placed))

    phase("pack")
    def pack_slab(j, carry):
        slab = ustate[pl.ds(pl.multiple_of(8 * j, 8), 8), :]
        usend[j] = jnp.concatenate([slab[:, 0:128], slab[:, 128:256]], axis=0).astype(BF16)
        return carry

    lax.fori_loop(0, NSP, pack_slab, 0)
    urecv[sp] = usend[sp]
    arecv[sp] = arow[...]
    nrecv[sp] = nrow[...]

    my_stage = jnp.where(sp < STAGES[1][0], 0, jnp.where(sp < STAGES[2][0], 1, 2))

    def b_copy(dst):
        return pltpu.make_async_remote_copy(
            src_ref=arow, dst_ref=arecv.at[sp], send_sem=bsem.at[0], recv_sem=bsem.at[1 + my_stage],
            device_id={"sp": dst, "tp": tp}, device_id_type=MESH,
        )

    def n_copy(dst):
        return pltpu.make_async_remote_copy(
            src_ref=nrow, dst_ref=nrecv.at[sp], send_sem=nsem.at[0], recv_sem=nsem.at[1],
            device_id={"sp": dst, "tp": tp}, device_id_type=MESH,
        )

    def u_copy(dst):
        return pltpu.make_async_remote_copy(
            src_ref=usend.at[dst], dst_ref=urecv.at[sp], send_sem=usem.at[0], recv_sem=usem.at[1 + my_stage],
            device_id={"sp": dst, "tp": tp}, device_id_type=MESH,
        )

    def s_copy(dst):
        return pltpu.make_async_remote_copy(
            src_ref=ssend.at[dst], dst_ref=srecv.at[sp], send_sem=ssem.at[0], recv_sem=ssem.at[1],
            device_id={"sp": dst, "tp": tp}, device_id_type=MESH,
        )

    def send_first():
        for n in range(NSP - 1):
            dst = sp_peer(n)
            b_copy(dst).start()
            u_copy(dst).start()
        for n in range(NSP - 1):
            n_copy(sp_peer(n)).start()

    def send_second(stage):
        first, size = STAGES[stage]
        for n in range(size):
            dst = first + lax.rem(sp + size // 2 + n, size)

            @pl.when(dst != sp)
            def _():
                s_copy(dst).start()

    def wait_first(stage):
        def wait(count):
            pltpu.make_async_copy(arecv.at[pl.ds(0, count)], arecv.at[pl.ds(0, count)], bsem.at[1 + stage]).wait()
            pltpu.make_async_copy(urecv.at[pl.ds(0, count)], urecv.at[pl.ds(0, count)], usem.at[1 + stage]).wait()

        @pl.when(my_stage == stage)
        def _():
            wait(STAGES[stage][1] - 1)

        @pl.when(my_stage != stage)
        def _():
            wait(STAGES[stage][1])

    phase("send1")
    send_first()
    w_copies = [
        pltpu.make_async_remote_copy(
            src_ref=src, dst_ref=dst, send_sem=wsend.at[i], recv_sem=wrecv.at[i], device_id=sib, device_id_type=MESH
        )
        for i, (src, dst) in enumerate([(w_out_memory, wom.at[pl.ds(H, H)]), (w_out_pool, wop.at[pl.ds(G, G)])])
    ]
    for copy in w_copies:
        copy.start()

    phase("pgate")
    for i in range(11, 17):
        copies[i].wait()
    for i in range(2):
        rows = pl.ds(512 * i, 512)
        pgate[rows, :] = silu(nn(nrm[rows, :], wpg[...])) * pg[...]

    def p_copy(n):
        return pltpu.make_async_remote_copy(
            src_ref=pbuf.at[2 * n + 1 - c], dst_ref=psib.at[n], send_sem=psem.at[0], recv_sem=psem.at[1],
            device_id=sib, device_id_type=MESH,
        )

    order = (2, 1, 3, 0)

    def rs_copy(n, src, dst, to):
        return pltpu.make_async_remote_copy(
            src_ref=src, dst_ref=dst, send_sem=rsend.at[0], recv_sem=rrecv.at[n], device_id=to, device_id_type=MESH
        )

    rs = [
        rs_copy(0, part.at[2, 0], r1, up), rs_copy(1, part.at[2, 1], r2, down),
        rs_copy(2, part.at[1, 1], r3, up), rs_copy(3, part.at[3, 0], r4, down),
        rs_copy(4, fwd.at[0], r5, up), rs_copy(5, fwd.at[1], r6, down),
        rs_copy(6, ppart.at[0], rp1, up), rs_copy(7, ppart.at[1], rp2, down),
    ]

    def memory_inputs(dy):
        to = lax.rem(y + dy, NY)
        return jnp.concatenate([zbuf[2 * to + c], zsib[to]], axis=1)

    def pool_inputs(dy):
        to = lax.rem(y + dy, NY)
        return jnp.concatenate([pbuf[2 * to + c], psib[to]], axis=1)

    phase("q")
    for i in range(2):
        rows = pl.ds(512 * i, 512)
        q[rows, :] = nn(nrm[rows, :], wq[...]).astype(BF16)

    memory = jnp.concatenate([im[:, 0:128], im[:, 128:256]], axis=0)
    stab = jnp.zeros((1, 1), F32)
    my_stab = jnp.zeros((1, 1), F32)
    steps = []
    best = scan_packed(offer, jnp.maximum, NEG)
    head_scale = H ** (-0.5)

    def beside():
        phase("pool")
        with_halo(sp > 0, lambda copy: copy.wait_recv())
        window = lax.shift_left(jnp.int32(2), tp)
        for i in range(4):
            rows = pl.ds(256 * i, 256)
            near = pool_ext[pl.ds(256 * i, 512), :]
            target = lax.broadcasted_iota(jnp.int32, (256, 512), 0) + HALO
            back = target - lax.broadcasted_iota(jnp.int32, (256, 512), 1)
            band = jnp.where((back >= 0) & (back < window), 1.0, 0.0).astype(BF16)
            sums = nn(band, near)
            place = sp * T + 256 * i + lax.broadcasted_iota(jnp.int32, (256, 1), 0) + 1
            count = jnp.minimum(place, window).astype(F32)
            pooled = (sums / count - near[HALO:, :].astype(F32)).astype(BF16)
            mixed = nn(pooled, pm[...]) * pgate[rows, :]
            pbuf[2 * i] = mixed[0:128].astype(BF16)
            pbuf[2 * i + 1] = mixed[128:256].astype(BF16)

        for n in range(NY):
            p_copy(n).start()

        phase("attn")
        colC = columns_of([best])
        for i in range(4):
            rows = pl.ds(256 * i, 256)
            length = 256 * (i + 1)
            scores = nt(q[rows, :], k[pl.ds(0, length), :])
            source = jnp.concatenate([offer[r : r + 1, :] for r in range(2 * (i + 1))], axis=1)
            exponent = source - column(colC, 0, i)
            ahead = lax.broadcasted_iota(jnp.int32, (256, length), 1) > lax.broadcasted_iota(
                jnp.int32, (256, length), 0
            ) + 256 * i
            weights = jnp.exp(jnp.where(ahead, NEG, exponent)) * scores * head_scale
            den[rows, :] = jnp.broadcast_to(jnp.sum(weights, axis=1, keepdims=True), (256, 128))
            num[rows, :] = nn(weights.astype(BF16), v[pl.ds(0, length), :])

    for stage, (first, size) in enumerate(STAGES):
        phase("wait1_%d" % stage)
        wait_first(stage)
        phase("scan%d" % stage)
        for j in range(first, first + size):
            mine = sp == j
            my_stab = jnp.where(mine, stab, my_stab)
            ssend[j] = memory.astype(BF16)
            piece_stab = arecv[j, :, 0:1]
            piece_keep = arecv[j, :, 32:33]
            new_stab = jnp.maximum(stab + piece_keep, piece_stab)
            fade = jnp.exp(stab + piece_keep - new_stab)
            weight = jnp.exp(piece_stab - new_stab)
            memory = fade * memory + weight * urecv[j].astype(F32)
            steps.append((fade, weight))
            stab = new_stab

        phase("send2_%d" % stage)

        @pl.when(my_stage == stage)
        def _():
            srecv[sp] = ssend[sp]

        send_second(stage)
        if stage == 0:
            phase("gate")
            for i in range(2):
                rows = pl.ds(512 * i, 512)
                gate[rows, :] = silu(nn(nrm[rows, :], wg[...])) * mg[...]
        if stage == 1:
            pl.when(sp < HALF)(beside)
    pl.when(sp >= HALF)(beside)

    phase("pout")
    for i in range(17, 20):
        copies[i].wait()
    for copy in w_copies:
        copy.wait_recv()
    pltpu.make_async_copy(psib, psib, psem.at[1]).wait()
    pool_in = pool_inputs(2)
    for quarter in range(4):
        at = pl.ds(512 * (quarter % 2), 512)
        ppart[quarter // 2, :, at] = nn(pool_in, wop[:, pl.ds(512 * quarter, 512)]).astype(BF16)
    rs[6].start()
    rs[7].start()

    phase("denom")
    pltpu.make_async_copy(nrecv.at[pl.ds(0, NSP - 1)], nrecv.at[pl.ds(0, NSP - 1)], nsem.at[1]).wait()
    quarters = []
    for first in range(0, NSP, 8):
        total = arecv[first]
        for j in range(first + 1, first + 8):
            total = total + arecv[j]
        quarters.append(total)
    my_n = jnp.concatenate(
        [jnp.where(lane128 < 64, pltpu.roll(quarters[n], 64, 1), quarters[n + 1]) for n in (0, 2)], axis=0
    )
    for j, (fade, weight) in enumerate(steps[: NSP - 1]):
        my_n = jnp.where(sp > j, fade * my_n + weight * nrecv[j], my_n)
    joint = jnp.maximum(best, my_stab)
    local_weight = jnp.exp(best - joint)
    carry_weight = jnp.exp(my_stab - joint) * head_scale
    least = jnp.exp(-(keep_run + joint))
    cols[...] = columns_of([local_weight, carry_weight, least])
    n_row = jnp.concatenate([my_n[0:1, :], my_n[1:2, :]], axis=1)
    n_top = n_row.astype(BF16)
    n_mid = (n_row - n_top.astype(F32)).astype(BF16)
    n_low = (n_row - n_top.astype(F32) - n_mid.astype(F32)).astype(BF16)
    n_rows = jnp.concatenate([n_top, n_mid, n_low, jnp.zeros((13, H), BF16)], axis=0)
    colB = cols[...]
    for i in range(4):
        rows = pl.ds(256 * i, 256)
        carried = jnp.sum(nt(q[rows, :], n_rows), axis=1, keepdims=True)
        full = den[rows, 0:1] * column(colB, 0, i) + column(colB, 1, i) * carried
        inverse = 1.0 / jnp.maximum(jnp.abs(full), column(colB, 2, i))
        num[rows, :] = num[rows, :] * (column(colB, 0, i) * inverse)
        den[rows, :] = jnp.broadcast_to(column(colB, 1, i) * inverse, (256, 128))

    phase("wait2")
    pltpu.make_async_copy(srecv.at[pl.ds(0, NSP - 1)], srecv.at[pl.ds(0, NSP - 1)], ssem.at[1]).wait()
    phase("finish")
    for j in range(NSP):
        slab = srecv[j].astype(F32)
        smat[8 * j : 8 * j + 8, 0:128] = slab[0:8]
        smat[8 * j : 8 * j + 8, 128:256] = slab[8:16]
    held = smat[...].astype(BF16)
    lane_sq = lax.broadcasted_iota(jnp.int32, (128, 128), 1)
    squares = jnp.zeros((128, 128), F32)

    def z_copy(n):
        to = lax.rem(y + order[n], NY)
        return pltpu.make_async_remote_copy(
            src_ref=zbuf.at[2 * to + 1 - c], dst_ref=zsib.at[to], send_sem=zsem.at[NY], recv_sem=zsem.at[n],
            device_id=sib, device_id_type=MESH,
        )

    z_copies = [z_copy(n) for n in range(NY)]
    for n in range(NY):
        for core in (1 - c, c):
            block = 2 * lax.rem(y + order[n], NY) + core
            rows = pl.ds(pl.multiple_of(128 * block, 128), 128)
            memory_rows = num[rows, :] + den[rows, 0:1] * nn(q[rows, :], held)
            sq = jnp.sum(memory_rows * memory_rows, axis=1, keepdims=True)
            squares = jnp.where(lane_sq == block, sq, squares)
            zbuf[block] = (memory_rows * gate[rows, :]).astype(BF16)
        z_copies[n].start()
    own_sq = squares.T[0:8]
    sqs[...] = own_sq

    def sq_copy(n):
        return pltpu.make_async_remote_copy(
            src_ref=sqs, dst_ref=sqr.at[n], send_sem=qsem.at[0], recv_sem=qsem.at[1],
            device_id={"sp": sp, "tp": lax.rem(tp + n + 1, NTP)}, device_id_type=MESH,
        )

    for n in range(NTP - 1):
        sq_copy(n).start()
    eye = lax.broadcasted_iota(jnp.int32, (128, 128), 0) == lax.broadcasted_iota(jnp.int32, (128, 128), 1)

    def out_scale(dy):
        to = lax.rem(y + dy, NY)
        row = cols[pl.ds(2 * to + c, 1), :]
        return jnp.sum(jnp.where(eye, jnp.broadcast_to(row, (128, 128)), 0.0), axis=1, keepdims=True)

    phase("zwait")
    z_copies[0].wait_recv()
    phase("ob2")
    memory_in = memory_inputs(2)
    for half in range(2):
        for quarter in range(2):
            at = pl.ds(512 * quarter, 512)
            part[2, half, :, at] = nn(memory_in, wom[:, pl.ds(1024 * half + 512 * quarter, 512)]).astype(BF16)
        rs[half].start()

    phase("sqwait")
    pltpu.make_async_copy(sqr, sqr, qsem.at[1]).wait()
    phase("scale")
    total = own_sq
    for n in range(NTP - 1):
        total = total + sqr[n]
    cols[0:8, :] = lax.rsqrt(total / (NTP * H) + EPS)
    for n, dy in ((1, 1), (2, 3), (3, 0)):
        phase("ob%d" % dy)
        z_copies[n].wait_recv()
        memory_in, pool_in = memory_inputs(dy), pool_inputs(dy)
        scale = out_scale(dy)
        for half in (1, 0) if dy == 1 else (0, 1):
            for quarter in range(2):
                at = pl.ds(1024 * half + 512 * quarter, 512)
                term = nn(memory_in, wom[:, at]) * scale + nn(pool_in, wop[:, at])
                part[dy, half, :, pl.ds(512 * quarter, 512)] = term.astype(BF16)
            if dy and half == dy % 3:
                rs[1 + dy - dy // 2].start()

    phase("drain")
    all_b = arecv.at[pl.ds(0, NSP - 1)]
    pltpu.make_async_copy(nrecv.at[pl.ds(0, NSP - 1)], nrecv.at[pl.ds(0, NSP - 1)], nsem.at[0]).wait()
    all_u = urecv.at[pl.ds(0, NSP - 1)]
    pltpu.make_async_copy(all_b, all_b, bsem.at[0]).wait()
    pltpu.make_async_copy(all_u, all_u, usem.at[0]).wait()
    pltpu.make_async_copy(all_u, all_u, ssem.at[0]).wait()
    for copy in w_copies:
        copy.wait_send()
    pltpu.make_async_copy(zsib, zsib, zsem.at[NY]).wait()

    with_halo(sp < NSP - 1, lambda copy: copy.wait_send())
    pltpu.make_async_copy(psib, psib, psem.at[0]).wait()
    pltpu.make_async_copy(sqr, sqr, qsem.at[0]).wait()
    rs[6].wait_recv()
    rs[7].wait_recv()

    phase("rw0")
    rs[0].wait_recv()
    phase("fwd0")
    fwd[0] = (part[1, 0].astype(F32) + rp1[...].astype(F32) + out_scale(1) * r1[...].astype(F32)).astype(BF16)
    rs[4].start()
    phase("rw1")
    rs[1].wait_recv()
    phase("fwd1")
    fwd[1] = (part[3, 1].astype(F32) + rp2[...].astype(F32) + out_scale(3) * r2[...].astype(F32)).astype(BF16)
    rs[5].start()
    phase("rw2")
    for n in range(2, 4):
        rs[n].wait_recv()
    low = part[0, 0].astype(F32) + r4[...].astype(F32)
    high = part[0, 1].astype(F32) + r3[...].astype(F32)
    phase("rw4")
    for n in range(4, 6):
        rs[n].wait_recv()
    phase("final")
    low = low + r5[...].astype(F32)
    high = high + r6[...].astype(F32)
    mean = (jnp.sum(low * low, axis=1, keepdims=True) + jnp.sum(high * high, axis=1, keepdims=True)) / D
    scale = lax.rsqrt(mean + EPS)
    out[:, 0:1024] = (low * scale * post[:, 0:1024]).astype(BF16)
    out[:, 1024:2048] = (high * scale * post[:, 1024:2048]).astype(BF16)
    pltpu.make_async_copy(part, part, rsend.at[0]).wait()
    phase(None)


def body(
    tokens, pre_gain, w_query, w_key, w_value, memory_output_gate_weight, w_input_gate, w_forget_gate, input_bias,
    forget_bias, forget_extra, initial_memory, initial_normal, memory_gain, w_pool_input, w_pool_gate, pool_mix,
    pool_gain, w_out_memory, w_out_pool, post_gain,
):
    args = (
        tokens, pre_gain.reshape(1, D), w_query, w_key, w_value, memory_output_gate_weight, w_input_gate.T,
        w_forget_gate.T, input_bias.reshape(1, 8), forget_bias.reshape(1, 8), forget_extra.reshape(8, 128),
        initial_memory.reshape(8, H), initial_normal, memory_gain.reshape(1, D), w_pool_input, w_pool_gate, pool_mix,
        pool_gain.reshape(1, NTP * G), w_out_memory, w_out_pool, post_gain.reshape(1, D),
    )
    vmem = pltpu.VMEM
    dma = pltpu.SemaphoreType.DMA
    scratch = [
        vmem((T, D), BF16), vmem((T, D), BF16), vmem((D, H), BF16), vmem((D, H), BF16), vmem((D, H), BF16),
        vmem((D, H), BF16), vmem((D, 2 * G), BF16), vmem((D, G), BF16), vmem((16, D), BF16), vmem((1, D), F32), vmem((1, 8), F32),
        vmem((1, 8), F32), vmem((8, 128), F32), vmem((8, H), F32), vmem((1, 8), F32), vmem((1, H), F32),
        vmem((G, G), BF16), vmem((1, G), F32), vmem((2 * H, D), BF16), vmem((2 * G, D), BF16), vmem((1, D), F32),
        vmem((T, 128), F32), vmem((T, H), BF16), vmem((T, H), BF16), vmem((T, H), BF16), vmem((T, H), F32),
        vmem((HALO + T, G), BF16), vmem((T, G), F32), vmem((T, H), F32), vmem((T, 128), F32), vmem((128, 128), F32),
        vmem((H, H), F32), vmem((NSP, 16, 128), BF16), vmem((NSP, 16, 128), BF16), vmem((1, 128), F32),
        vmem((NSP, 1, 128), F32), vmem((2, 128), F32), vmem((NSP, 2, 128), F32), vmem((NSP, 16, 128), BF16), vmem((NSP, 16, 128), BF16), vmem((H, H), F32),
        vmem((8, 128), F32), vmem((NTP - 1, 8, 128), F32), vmem((NTP, 128, H), BF16), vmem((NY, 128, H), BF16),
        vmem((NTP, 128, G), BF16), vmem((NY, 128, G), BF16),
        vmem((2, 128, 1024), BF16), vmem((NY, 2, 128, 1024), BF16), vmem((2, 128, 1024), BF16), vmem((128, 1024), BF16), vmem((128, 1024), BF16),
        vmem((128, 1024), BF16), vmem((128, 1024), BF16), vmem((128, 1024), BF16), vmem((128, 1024), BF16),
        vmem((128, 1024), BF16), vmem((128, 1024), BF16),
        dma((20,)), dma((5,)), dma((2,)), dma((2,)), dma((4,)), dma((4,)), dma((2,)), dma((2,)), dma((2,)), dma((2,)),
        dma((NY + 1,)), dma((2,)), dma((1,)), dma((8,)),
    ]
    anywhere = pl.BlockSpec(memory_space=pltpu.HBM)
    return pl.pallas_call(
        kernel,
        out_shape=jax.ShapeDtypeStruct((128, D), BF16),
        in_specs=[anywhere] * len(args),
        out_specs=pl.BlockSpec(memory_space=pltpu.VMEM),
        scratch_shapes=scratch,
        compiler_params=pltpu.CompilerParams(
            collective_id=0, has_side_effects=True, vmem_limit_bytes=48 * 1024 * 1024
        ),
    )(*[pltpu.with_memory_space_constraint(a, pltpu.HBM) for a in args])


def solution(mesh):
    in_specs = (
        P("sp", None), P(), P(None, "tp"), P(None, "tp"), P(None, "tp"), P(None, "tp"), P(), P(), P(), P(),
        P("sp", "tp"), P("tp", "sp", None), P("tp", "sp"), P(), P(None, "tp"), P(None, "tp"), P(), P(),
        P("tp", None), P("tp", None), P(),
    )
    return jax.shard_map(
        body, mesh=mesh, in_specs=in_specs, out_specs=P(("sp", "tp"), None), check_vma=False
    )
```
